128 devices in a mesh: sp: 32 (over z, y, core), tp: 4 (over x).
Axes of the slice: x: 4, y: 4, z: 4, core: 2. Of those that a mesh axis runs over, the one named last changes fastest.
Arguments:
- residual_in: bfloat16 [32768, 2048], P(('sp', 'tp')), may hold values from -6 to 6
- queries: bfloat16 [32768, 2048], P('sp', 'tp'), may hold values from -200 to 200, as said below
- keys_values: bfloat16 [2, 32768, 1024], P(None, 'sp', 'tp'), may hold values from -6 to 6
- sink_logit: float32 [32], P('tp'), may hold values from -2 to 6
- out_weight: bfloat16 [2048, 2048], P('tp'), may hold values from -2 to 2
- norm1_gain: float32 [2048], replicated, may hold values from 0.1 to 1.9
- norm1_bias: float32 [2048], replicated, may hold values from -3 to 3
- up_weight: bfloat16 [2048, 8192], P('sp', 'tp'), may hold values from -0.125 to 0.125
- down_weight: bfloat16 [8192, 2048], P('tp', 'sp'), may hold values from -0.0625 to 0.0625
- norm2_gain: float32 [2048], replicated, may hold values from 0.1 to 1.9
- norm2_bias: float32 [2048], replicated, may hold values from -3 to 3
Outputs:
- stream_out: bfloat16 [32768, 2048], P(('sp', 'tp'))
The draws below stay inside these ranges and needn't reach their ends.
Inputs may be any that keep to these rules, and one draw needn't show every extreme that they name: `queries`: of order one mostly; some rows may be large multiples of a nearby key row.
All inputs are finite; a program needn't handle non-finite values.
Results may differ from the reference program's by a relative error of at most 0.014.
Values may be sent and summed in bfloat16 or wider, within the bound.
A program may use at most 128 MiB of HBM per device.

```python
import jax
import jax.numpy as jnp
from jax import lax

D = 2048
HEADS = 32
KV_HEADS = 16
HEAD_DIM = 64
FF = 8192
WINDOW = 128
TOK_DEV = 1024
TOKENS = 32768
N_TP = 4


def joint_draw(key):
    query = jnp.clip(jax.random.normal(jax.random.fold_in(key, 11), (TOKENS, HEADS * HEAD_DIM), jnp.float32), -5.0, 5.0)
    pairs = jnp.clip(jax.random.normal(jax.random.fold_in(key, 12), (2, TOKENS, KV_HEADS * HEAD_DIM), jnp.float32), -5.0, 5.0)
    return (query, pairs)


def draw_queries(key, part):
    return joint_draw(key)[0].astype(jnp.bfloat16)


def draw_keys_values(key, part):
    return joint_draw(key)[1].astype(jnp.bfloat16)


def levels(key, extent, split, low, top_value):
    level = 1.0
    for dim, shards_of in split:
        heights = jax.random.uniform(jax.random.fold_in(jax.random.fold_in(key, 6), dim), (shards_of,), jnp.float32, low / len(split), top_value / len(split))
        level = level * jnp.repeat(jnp.exp(heights), extent[dim] // shards_of).reshape((-1,) + (1,) * (len(extent) - 1 - dim))
    return level


def noise(rng, extent, width, most, split=(), kind=jnp.bfloat16):
    factor_of = levels(rng, extent, split, -0.22, 0.18) if split else 1.0
    values = jax.random.normal(rng, extent, jnp.float32) * width * factor_of
    return jnp.minimum(jnp.maximum(values, -most), most).astype(kind)


def setup_inputs(seed: int = 0) -> dict:
    splits = jax.random.split(jax.random.key(seed), 12)
    residual_in = noise(splits[0], (TOKENS, D), 1.0, 6.0, ((0, 128),))
    queries = draw_queries(jax.random.fold_in(splits[11], 71), 0)
    keys_values = draw_keys_values(jax.random.fold_in(splits[11], 71), 0)
    sink_logit = jnp.clip(-2.0 + 8.0 * jax.random.uniform(splits[3], (HEADS,), jnp.float32) ** levels(splits[3], (HEADS,), ((0, 4),), -0.2, 0.2), -2.0, 6.0)
    out_weight = noise(splits[4], (HEADS * HEAD_DIM, D), (6 * (HEADS * HEAD_DIM) ** -0.5), 2.0, ((0, 4),))
    norm1_gain = jnp.clip(1.0 + 0.18 * jax.random.normal(splits[5], (D,), jnp.float32), 0.1, 1.9)
    norm1_bias = noise(splits[6], (D,), 0.3, 3.0, (), jnp.float32)
    up_weight = noise(splits[7], (D, FF), D ** -0.5, 0.125, ((0, 32), (1, 4)))
    down_weight = noise(splits[8], (FF, D), FF ** -0.5, 0.0625, ((0, 4), (1, 32)))
    norm2_gain = jnp.clip(1.0 + 0.18 * jax.random.normal(splits[9], (D,), jnp.float32), 0.1, 1.9)
    norm2_bias = noise(splits[10], (D,), 0.3, 3.0, (), jnp.float32)
    return dict(residual_in=residual_in, queries=queries, keys_values=keys_values, sink_logit=sink_logit, out_weight=out_weight, norm1_gain=norm1_gain, norm1_bias=norm1_bias, up_weight=up_weight, down_weight=down_weight, norm2_gain=norm2_gain, norm2_bias=norm2_bias)


def norm_rows(values, gain, bias):
    mean = lax.optimization_barrier(jnp.mean(values, axis=-1, keepdims=True))
    centred = values - mean
    variance = lax.optimization_barrier(jnp.mean(centred * centred, axis=-1, keepdims=True))
    return (centred * lax.rsqrt(variance + 1e-06) * gain + bias).astype(jnp.bfloat16)

def reference(residual_in, queries, keys_values, sink_logit, out_weight, norm1_gain, norm1_bias, up_weight, down_weight, norm2_gain, norm2_bias):
    block = min(512, TOK_DEV)
    span = block + 2 * WINDOW
    group = HEADS // KV_HEADS
    padded = jnp.pad(keys_values, ((0, 0), (WINDOW, WINDOW), (0, 0)))
    sink = sink_logit.reshape(KV_HEADS, group, 1, 1)

    def one_block(index):
        start = (index * block).astype(jnp.int32)
        query = lax.dynamic_slice_in_dim(queries, start, block, 0).astype(jnp.float32).reshape(block, KV_HEADS, group, HEAD_DIM)
        keys = lax.dynamic_slice_in_dim(padded[0], start, span, 0).astype(jnp.float32).reshape(span, KV_HEADS, HEAD_DIM)
        values = lax.dynamic_slice_in_dim(padded[1], start, span, 0).astype(jnp.float32).reshape(span, KV_HEADS, HEAD_DIM)
        scores = jnp.einsum('qhgd,khd->hgqk', query, keys) * HEAD_DIM ** (-0.5)
        query_pos = start + jnp.arange(block, dtype=jnp.int32)
        key_pos = start - WINDOW + jnp.arange(span, dtype=jnp.int32)
        valid = (jnp.abs(key_pos[None, :] - query_pos[:, None]) <= WINDOW) & (key_pos[None, :] >= 0) & (key_pos[None, :] < TOKENS)
        scores = jnp.where(valid, scores, -jnp.inf)
        top = jnp.maximum(lax.optimization_barrier(jnp.max(scores, axis=-1, keepdims=True)), sink)
        expd = jnp.exp(scores - top)
        total = lax.optimization_barrier(jnp.sum(expd, axis=-1, keepdims=True)) + jnp.exp(sink - top)
        weights = lax.optimization_barrier((expd / total).astype(jnp.bfloat16)).astype(jnp.float32)
        mixed = jnp.einsum('hgqk,khd->qhgd', weights, values)
        return mixed.reshape(block, HEADS * HEAD_DIM).astype(jnp.bfloat16)
    attended = lax.map(one_block, jnp.arange(TOKENS // block, dtype=jnp.int32)).reshape(TOKENS, HEADS * HEAD_DIM)
    head_cols = HEADS * HEAD_DIM // N_TP
    projected = jnp.zeros((TOKENS, D), jnp.float32)
    for part in range(N_TP):
        term = jnp.dot(attended[:, part * head_cols:(part + 1) * head_cols], out_weight[part * head_cols:(part + 1) * head_cols], preferred_element_type=jnp.float32)
        projected = projected + term.astype(jnp.bfloat16).astype(jnp.float32)
    first = norm_rows(residual_in.astype(jnp.float32) + projected, norm1_gain, norm1_bias)
    hidden = jnp.dot(first, up_weight, preferred_element_type=jnp.float32)
    activation = jnp.square(jnp.maximum(hidden, 0.0)).astype(jnp.bfloat16)
    unit_cols = FF // N_TP
    branch = jnp.zeros((TOKENS, D), jnp.float32)
    for part in range(N_TP):
        term = jnp.dot(activation[:, part * unit_cols:(part + 1) * unit_cols], down_weight[part * unit_cols:(part + 1) * unit_cols], preferred_element_type=jnp.float32)
        branch = branch + term.astype(jnp.bfloat16).astype(jnp.float32)
    return norm_rows(first.astype(jnp.float32) + branch, norm2_gain, norm2_bias)
```

```python
import functools

import jax
import jax.numpy as jnp
from jax import lax
from jax.experimental import pallas as pl
from jax.experimental.pallas import tpu as pltpu
from jax.sharding import PartitionSpec as P

HEAD_DIM = 64
WINDOW = 128
BLOCK = 128
MESH = pl.DeviceIdType.MESH
F32 = jnp.float32
BF16 = jnp.bfloat16
ALL = slice(None)


def norm_rows(values, gain, bias):
    mean = jnp.mean(values, axis=-1, keepdims=True)
    centred = values - mean
    variance = jnp.mean(centred * centred, axis=-1, keepdims=True)
    return (centred * lax.rsqrt(variance + 1e-06) * gain + bias).astype(BF16)


def aligned(index, size):
    return pl.multiple_of(index * size, size)


class Links:
    def __init__(self, send, recv):
        self.send, self.recv, self.count, self.started = send, recv, 0, []

    def take(self):
        self.count += 1
        return self.count - 1

    def copy(self, src, dst, ident, target):
        return pltpu.make_async_remote_copy(
            src_ref=src,
            dst_ref=dst,
            send_sem=self.send.at[ident],
            recv_sem=self.recv.at[ident],
            device_id=target,
            device_id_type=MESH,
        )

    def start(self, src, dst, ident, target, again=None):
        self.copy(src, dst, ident, target).start()
        self.started.append((again or (lambda: src), ident, target))

    def arrived(self, dst, ident, target):
        self.copy(dst, dst, ident, target).wait_recv()

    def finish(self):
        for again, ident, target in self.started:
            src = again()
            self.copy(src, src, ident, target).wait_send()


class Spread:
    def __init__(self, links, part, first, second, core, peers, sister):
        self.links, self.part, self.core, self.sister = links, part, core, sister
        self.own1, self.own2 = first, second
        self.up1, self.down1, self.up2, self.down2 = peers
        self.ids = [links.take() for _ in range(12)]
        self.near1 = [(first + hop) % 4 for hop in (3, 1, 2)]
        self.near2 = [(second + hop) % 4 for hop in (3, 1, 2)]

    def at(self, one, two, sub=None, core=None):
        return self.part(one, two, self.core if core is None else core, sub)

    def push(self, ident, target, one, two, sub=None, source=None):
        place = self.at(one, two, sub)
        again = (lambda: self.at(one, two, sub)) if source is None else (lambda: source)
        src = place if source is None else source
        self.links.start(src, place, self.ids[ident], target, again)

    def pull(self, ident, target, one, two, sub=None, core=None):
        self.links.arrived(self.at(one, two, sub, core), self.ids[ident], target)

    def step1(self):
        self.push(0, self.up1, self.own1, self.own2)
        self.push(1, self.down1, self.own1, self.own2)

    def step2(self):
        before, after, _ = self.near1
        self.pull(0, self.up1, before, self.own2)
        self.push(2, self.up1, before, self.own2, 0)
        self.pull(1, self.down1, after, self.own2)
        self.push(3, self.down1, after, self.own2, 1)

    def step3(self):
        across = self.near1[2]
        self.pull(2, self.up1, across, self.own2, 0)
        self.pull(3, self.down1, across, self.own2, 1)
        self.push(4, self.up2, ALL, self.own2)
        self.push(5, self.down2, ALL, self.own2)
        self.push(8, self.sister, ALL, self.own2)

    def step4(self):
        before, after, _ = self.near2
        self.pull(4, self.up2, ALL, before)
        self.push(6, self.up2, ALL, before, 0)
        self.pull(5, self.down2, ALL, after)
        self.push(7, self.down2, ALL, after, 1)
        self.push(9, self.sister, ALL, before)
        self.push(10, self.sister, ALL, after)

    def step5(self):
        across = self.near2[2]
        self.pull(6, self.up2, ALL, across, 0)
        self.pull(7, self.down2, ALL, across, 1)
        self.push(11, self.sister, ALL, across)

    def step6(self):
        for place, ident in zip([self.own2] + self.near2, (8, 9, 10, 11)):
            self.pull(ident, self.sister, ALL, place, None, 1 - self.core)


def layer_kernel(
    total, res_h, q_h, kv_h, sink_ref, ow_h, g1_ref, b1_ref, up_h, dn_h, g2_ref, b2_ref, out_h,
    qv, kvv, att, attr, resv, oww, upw, dnw, raw, slab, rows, act, pre, part, own, rin, rfin, outv,
    local, send, recv, asend, arecv,
):
    sp, x = lax.axis_index("sp"), lax.axis_index("tp")
    core, chip = sp % 2, sp // 2
    y, z = chip % 4, chip // 4

    def device(zi, yi, ci, xi):
        return {"sp": ((zi % 4) * 4 + yi % 4) * 2 + ci, "tp": xi % 4}

    sister = device(z, y, 1 - core, x)
    right, left, across = (device(z, y, core, x + d) for d in (1, 3, 2))
    yup, ydown = device(z, y + 1, core, x), device(z, y + 3, core, x)
    zup, zdown = device(z + 1, y, core, x), device(z + 3, y, core, x)
    later, earlier = {"sp": (sp + 1) % 32, "tp": x}, {"sp": (sp + 31) % 32, "tp": x}

    loads = []

    def load(src, dst):
        copy = pltpu.make_async_copy(src, dst, local.at[len(loads)])
        copy.start()
        loads.append(copy)
        return copy

    kv_copy = load(kv_h, kvv.at[:, pl.ds(WINDOW, 1024), :])
    q_copy = load(q_h, qv)
    ow_copy = load(ow_h, oww.at[0])
    up_copy = load(up_h, upw.at[z, y, core])
    raw_copy = load(dn_h.at[pl.ds(aligned(core, 1024), 1024)], raw.at[0])
    res_copy = load(res_h, resv)

    barrier = pltpu.get_barrier_semaphore()
    far = {"sp": (sp + 31 + 2 * core) % 32, "tp": x}
    friends = (sister, right, left, across, yup, ydown, zup, zdown, far)
    for friend in friends:
        pl.semaphore_signal(barrier, inc=1, device_id=friend, device_id_type=MESH)
    pl.semaphore_wait(barrier, len(friends))

    links = Links(send, recv)
    halo = [links.take() for _ in range(2)]
    links.start(
        kv_h.at[:, pl.ds(1024 - WINDOW, WINDOW), :], kvv.at[:, pl.ds(0, WINDOW), :], halo[0], later
    )
    links.start(
        kv_h.at[:, pl.ds(0, WINDOW), :], kvv.at[:, pl.ds(1024 + WINDOW, WINDOW), :], halo[1], earlier
    )

    seed = [links.take() for _ in range(3)]
    seeds = ((right, 3), (left, 1), (across, 2))
    for ident, (target, place) in zip(seed, seeds):
        links.start(ow_h.at[z, y, core], oww.at[place, z, y, core], ident, target)

    def ow_part(half, flip):
        def part_at(one, two, ci, sub):
            zi, yi = (two, one) if flip else (one, two)
            at, wide = half * 1024, 1024
            if sub is not None:
                at, wide = at + sub * 512, 512
            return oww.at[pl.ds(1, 3), zi, yi, ci, :, pl.ds(at, wide)]

        return part_at

    def up_part(half, flip):
        def part_at(one, two, ci, sub):
            zi, yi = (two, one) if flip else (one, two)
            span = pl.ds(0, 64) if sub is None else pl.ds(sub * 32, 32)
            return upw.at[zi, yi, ci, span, pl.ds(half * 1024, 1024)]

        return part_at

    def dn_part(half, flip):
        def part_at(one, two, ci, sub):
            zi, yi = (two, one) if flip else (one, two)
            at, tall = half * 512, 512
            if sub is not None:
                at, tall = at + sub * 256, 256
            span = pl.ds(pl.multiple_of(ci * 1024 + at, 256), tall)
            lanes = ALL if isinstance(yi, slice) else pl.ds(aligned(yi, 128), 128)
            return dnw.at[zi, span, lanes]

        return part_at

    def spread(make):
        return (
            Spread(links, make(0, False), z, y, core, (zup, zdown, yup, ydown), sister),
            Spread(links, make(1, True), y, z, core, (yup, ydown, zup, zdown), sister),
        )

    outs, ups, downs = spread(ow_part), spread(up_part), spread(dn_part)

    def run(pair, step):
        for one in pair:
            getattr(one, f"step{step}")()

    swap = links.take()
    links.start(dn_h.at[pl.ds(aligned(1 - core, 1024), 1024)], raw.at[1], swap, sister)

    for ident, (target, place) in zip(seed, seeds):
        links.arrived(oww.at[place, z, y, core], ident, target)
    run(outs, 1)
    up_copy.wait()
    run(ups, 1)

    def build_slab():
        raw_copy.wait()
        links.arrived(raw.at[1], swap, sister)

        def body(i, carry):
            span = pl.ds(aligned(i, 128), 128)
            mine, other = raw[0, span, :], raw[1, span, :]
            first = core == 0
            slab[span, 0:64] = jnp.where(first, mine, other)
            slab[span, 64:128] = jnp.where(first, other, mine)
            there = pl.ds(pl.multiple_of(core * 1024 + i * 128, 128), 128)
            dnw[z, there, pl.ds(aligned(y, 128), 128)] = slab[span, :]
            return carry

        lax.fori_loop(0, 8, body, 0)

    q_copy.wait()
    kv_copy.wait()
    span = BLOCK + 2 * WINDOW
    iota_r = lax.broadcasted_iota(jnp.int32, (BLOCK, span), 0)
    iota_c = lax.broadcasted_iota(jnp.int32, (BLOCK, span), 1)

    def block_copy(index, half, step, target):
        return pltpu.make_async_remote_copy(
            src_ref=att.at[index],
            dst_ref=attr.at[half, :, pl.ds(aligned(3 - step, 512), 512)],
            send_sem=asend.at[half, step],
            recv_sem=arecv.at[half, step],
            device_id=target,
            device_id_type=MESH,
        )

    events = {
        2: lambda: run(outs + ups, 2),
        3: build_slab,
        4: lambda: run(outs, 3),
        6: lambda: run(downs, 1),
    }

    def attend(index, carry):
        half, step = index // 4, index % 4
        owner = (x + 1 + step) % 4
        block = 2 * owner + half

        @pl.when(block == 0)
        def _():
            links.arrived(kvv.at[:, pl.ds(0, WINDOW), :], halo[0], later)

        @pl.when(block == 7)
        def _():
            links.arrived(kvv.at[:, pl.ds(1024 + WINDOW, WINDOW), :], halo[1], earlier)

        begin = aligned(block, BLOCK)
        pos = iota_c + (sp * 1024 + block * BLOCK - WINDOW)
        gap = iota_c - iota_r
        valid = (gap >= 0) & (gap <= 2 * WINDOW) & (pos >= 0) & (pos < total)
        for kv in range(4):
            lanes = slice(kv * HEAD_DIM, (kv + 1) * HEAD_DIM)
            keys = kvv[0, pl.ds(begin, span), lanes]
            values = kvv[1, pl.ds(begin, span), lanes]
            for sub in range(2):
                head = kv * 2 + sub
                mine = slice(head * HEAD_DIM, (head + 1) * HEAD_DIM)
                query = qv[pl.ds(begin, BLOCK), mine]
                scores = lax.dot_general(
                    query, keys, (((1,), (1,)), ((), ())), preferred_element_type=F32
                ) * HEAD_DIM ** (-0.5)
                scores = jnp.where(valid, scores, -jnp.inf)
                sink = sink_ref[head]
                top = jnp.maximum(jnp.max(scores, axis=-1, keepdims=True), sink)
                expd = jnp.exp(scores - top)
                denom = jnp.sum(expd, axis=-1, keepdims=True) + jnp.exp(sink - top)
                weights = (expd * (1.0 / denom)).astype(BF16)
                mixed = jnp.dot(weights, values, preferred_element_type=F32)
                att[index, :, mine] = mixed.astype(BF16)

        @pl.when(step < 3)
        def _():
            block_copy(index, half, step, {"sp": sp, "tp": owner}).start()

        @pl.when(step == 3)
        def _():
            attr[half, :, 0:512] = att[index]

        for when, event in events.items():
            pl.when(index == when)(event)
        return carry

    lax.fori_loop(0, 8, attend, 0)

    def peer(step):
        return (right, across, left)[step]

    gather = [[links.take() for _ in range(6)] for _ in range(2)]
    low, high = pl.ds(0, 64), pl.ds(64, 64)

    def project(half):
        for step in range(3):
            block_copy(4 * half + step, half, step, peer(step)).wait_recv()

        def body(n, carry):
            cols = pl.ds(aligned(n, 256), 256)
            weight = oww[:, :, :, :, :, cols].reshape(2048, 256)
            term = jnp.dot(attr[half], weight, preferred_element_type=F32)
            pre[:, cols] = term + resv[half * 128 : half * 128 + 128, cols].astype(F32)
            return carry

        lax.fori_loop(0, 8, body, 0)

        def norm(i, carry):
            some = pl.ds(aligned(i, 32), 32)
            rows[half, 0, some, :] = norm_rows(pre[some, :], g1_ref[...], b1_ref[...])
            return carry

        lax.fori_loop(0, 4, norm, 0)
        ids = gather[half]
        links.start(rows.at[half, 0, low], rows.at[half, 3, low], ids[0], right)
        links.start(rows.at[half, 0, high], rows.at[half, 1, high], ids[1], left)
        links.start(rows.at[half, 0, high], rows.at[half, 3, high], ids[2], right)
        links.start(rows.at[half, 0, low], rows.at[half, 1, low], ids[3], left)

    def pass_on(half):
        ids = gather[half]
        links.arrived(rows.at[half, 3, low], ids[0], right)
        links.start(rows.at[half, 3, low], rows.at[half, 2, low], ids[4], right)
        links.arrived(rows.at[half, 1, high], ids[1], left)
        links.start(rows.at[half, 1, high], rows.at[half, 2, high], ids[5], left)

    def gathered(half):
        ids = gather[half]
        links.arrived(rows.at[half, 3, high], ids[2], right)
        links.arrived(rows.at[half, 1, low], ids[3], left)
        links.arrived(rows.at[half, 2, low], ids[4], right)
        links.arrived(rows.at[half, 2, high], ids[5], left)

    def up_project(half):
        def body(n, carry):
            cols = pl.ds(aligned(n, 256), 256)
            weight = upw[:, :, :, :, cols].reshape(2048, 256)
            hidden = jnp.dot(
                rows[half].reshape(512, 2048), weight, preferred_element_type=F32
            )
            act[:, cols] = jnp.square(jnp.maximum(hidden, 0.0)).astype(BF16)
            return carry

        lax.fori_loop(0, 8, body, 0)

    scatter = [[links.take() for _ in range(6)] for _ in range(2)]

    def down_project(half):
        def body(n, carry):
            cols = pl.ds(aligned(n, 256), 256)
            weight = dnw[n // 2, :, pl.ds(aligned(n % 2, 256), 256)]
            term = jnp.dot(act[...], weight, preferred_element_type=F32)
            own[half, :, cols] = term[0:128]
            for r in range(1, 4):
                part[half, r - 1, :, cols] = term[r * 128 : r * 128 + 128].astype(BF16)
            return carry

        lax.fori_loop(0, 8, body, 0)
        ids = scatter[half]
        links.start(part.at[half, 1, low], rin.at[half, 0], ids[0], right)
        links.start(part.at[half, 1, high], rin.at[half, 1], ids[1], left)
        links.start(part.at[half, 0, high], rfin.at[half, 0, high], ids[2], right)
        links.start(part.at[half, 2, low], rfin.at[half, 1, low], ids[3], left)

    def join(half):
        ids = scatter[half]
        for side, (target, index, at) in enumerate(((right, 0, 0), (left, 2, 64))):
            links.arrived(rin.at[half, side], ids[side], target)
            span = pl.ds(at, 64)
            part[half, index, span, :] = (
                part[half, index, span, :].astype(F32) + rin[half, side].astype(F32)
            ).astype(BF16)
            links.start(
                part.at[half, index, span], rfin.at[half, side, span], ids[4 + side], target
            )

    stores = []

    def final(half):
        ids = scatter[half]
        links.arrived(rfin.at[half, 0, high], ids[2], right)
        links.arrived(rfin.at[half, 1, low], ids[3], left)
        links.arrived(rfin.at[half, 0, low], ids[4], right)
        links.arrived(rfin.at[half, 1, high], ids[5], left)

        def norm(i, carry):
            some = pl.ds(aligned(i, 32), 32)
            value = rows[half, 0, some, :].astype(F32) + own[half, some, :]
            value = value + rfin[half, 0, some, :].astype(F32)
            value = value + rfin[half, 1, some, :].astype(F32)
            outv[half, some, :] = norm_rows(value, g2_ref[...], b2_ref[...])
            return carry

        lax.fori_loop(0, 4, norm, 0)
        copy = pltpu.make_async_copy(
            outv.at[half], out_h.at[pl.ds(half * 128, 128)], local.at[6 + half]
        )
        copy.start()
        stores.append(copy)

    run(outs, 4)
    run(ups, 3)
    run(downs, 2)
    run(outs, 5)
    run(outs, 6)
    ow_copy.wait()
    res_copy.wait()
    project(0)
    project(1)
    run(ups, 4)
    run(downs, 3)
    pass_on(0)
    run(ups, 5)
    run(ups, 6)
    gathered(0)
    up_project(0)
    run(downs, 4)
    pass_on(1)
    run(downs, 5)
    run(downs, 6)
    down_project(0)
    gathered(1)
    up_project(1)
    join(0)
    down_project(1)
    final(0)
    join(1)
    final(1)
    links.finish()
    for half in range(2):
        for step in range(3):
            block_copy(4 * half + step, half, step, peer(step)).wait_send()
    for copy in stores:
        copy.wait()


def on_device(res, q, kv, sink, ow, g1, b1, up, dn, g2, b2):
    total = q.shape[0] * lax.axis_size("sp")
    hbm = pl.BlockSpec(memory_space=pl.ANY)
    vmem = pl.BlockSpec(memory_space=pltpu.VMEM)
    smem = pl.BlockSpec(memory_space=pltpu.SMEM)
    return pl.pallas_call(
        functools.partial(layer_kernel, total),
        in_specs=[hbm, hbm, hbm, smem, hbm, vmem, vmem, hbm, hbm, vmem, vmem],
        out_specs=hbm,
        out_shape=jax.ShapeDtypeStruct((256, 2048), BF16),
        scratch_shapes=[
            pltpu.VMEM((1024, 512), BF16),
            pltpu.VMEM((2, 1024 + 2 * WINDOW, 256), BF16),
            pltpu.VMEM((8, 128, 512), BF16),
            pltpu.VMEM((2, 128, 2048), BF16),
            pltpu.VMEM((256, 2048), BF16),
            pltpu.VMEM((4, 4, 4, 2, 16, 2048), BF16),
            pltpu.VMEM((4, 4, 2, 64, 2048), BF16),
            pltpu.VMEM((4, 2048, 512), BF16),
            pltpu.VMEM((2, 1024, 64), BF16),
            pltpu.VMEM((1024, 128), BF16),
            pltpu.VMEM((2, 4, 128, 2048), BF16),
            pltpu.VMEM((512, 2048), BF16),
            pltpu.VMEM((128, 2048), F32),
            pltpu.VMEM((2, 3, 128, 2048), BF16),
            pltpu.VMEM((2, 128, 2048), F32),
            pltpu.VMEM((2, 2, 64, 2048), BF16),
            pltpu.VMEM((2, 2, 128, 2048), BF16),
            pltpu.VMEM((2, 128, 2048), BF16),
            pltpu.SemaphoreType.DMA((8,)),
            pltpu.SemaphoreType.DMA((128,)),
            pltpu.SemaphoreType.DMA((128,)),
            pltpu.SemaphoreType.DMA((2, 3)),
            pltpu.SemaphoreType.DMA((2, 3)),
        ],
        compiler_params=pltpu.CompilerParams(
            collective_id=0, has_side_effects=True, vmem_limit_bytes=62 * 2**20
        ),
        cost_estimate=pl.CostEstimate(
            flops=2 * 10**10, bytes_accessed=24 * 2**20, transcendentals=4 * 10**6
        ),
        name="layer",
    )(
        res, q, kv, sink, ow.reshape(4, 4, 2, 16, 2048), g1.reshape(1, -1), b1.reshape(1, -1),
        up, dn, g2.reshape(1, -1), b2.reshape(1, -1),
    )


def solution(mesh):
    return jax.shard_map(
        on_device,
        mesh=mesh,
        in_specs=(
            P(("sp", "tp"), None),
            P("sp", "tp"),
            P(None, "sp", "tp"),
            P("tp"),
            P("tp", None),
            P(),
            P(),
            P("sp", "tp"),
            P("tp", "sp"),
            P(),
            P(),
        ),
        out_specs=P(("sp", "tp"), None),
        check_vma=False,
    )
```

```python
import functools

import jax
import jax.numpy as jnp
from jax import lax
from jax.experimental import pallas as pl
from jax.experimental.pallas import tpu as pltpu
from jax.sharding import PartitionSpec as P

HEAD_DIM = 64
WINDOW = 128
BLOCK = 128
XPART = 512
MESH = pl.DeviceIdType.MESH
F32 = jnp.float32
BF16 = jnp.bfloat16
ALL = slice(None)


def norm_rows(values, gain, bias):
    mean = jnp.mean(values, axis=-1, keepdims=True)
    centred = values - mean
    variance = jnp.mean(centred * centred, axis=-1, keepdims=True)
    return (centred * lax.rsqrt(variance + 1e-06) * gain + bias).astype(BF16)


def aligned(index, size):
    return pl.multiple_of(index * size, size)


class Links:
    def __init__(self, send, recv):
        self.send, self.recv, self.count, self.started = send, recv, 0, []

    def take(self):
        self.count += 1
        return self.count - 1

    def copy(self, src, dst, ident, target):
        return pltpu.make_async_remote_copy(
            src_ref=src,
            dst_ref=dst,
            send_sem=self.send.at[ident],
            recv_sem=self.recv.at[ident],
            device_id=target,
            device_id_type=MESH,
        )

    def start(self, src, dst, ident, target, again=None):
        self.copy(src, dst, ident, target).start()
        self.started.append((again or (lambda: src), ident, target))

    def arrived(self, dst, ident, target):
        self.copy(dst, dst, ident, target).wait_recv()

    def finish(self, keep=0):
        count = len(self.started) - keep
        for again, ident, target in self.started[:count]:
            src = again()
            self.copy(src, src, ident, target).wait_send()
        self.started = self.started[count:]


class Spread:
    def __init__(self, links, part, first, second, core, peers, sister):
        self.links, self.part, self.core, self.sister = links, part, core, sister
        self.own1, self.own2 = first, second
        self.up1, self.down1, self.up2, self.down2 = peers
        self.ids = [links.take() for _ in range(12)]
        self.near1 = [(first + hop) % 4 for hop in (3, 1, 2)]
        self.near2 = [(second + hop) % 4 for hop in (3, 1, 2)]

    def at(self, one, two, sub=None, core=None):
        return self.part(one, two, self.core if core is None else core, sub)

    def push(self, ident, target, one, two, sub=None):
        place = self.at(one, two, sub)
        self.links.start(place, place, self.ids[ident], target, lambda: self.at(one, two, sub))

    def share(self, ident, two):
        for one in range(4):
            place = self.at(one, two)
            self.links.copy(place, place, self.ids[ident], self.sister).start()
        self.links.started.append((lambda: self.at(ALL, two), self.ids[ident], self.sister))

    def pull(self, ident, target, one, two, sub=None, core=None):
        self.links.arrived(self.at(one, two, sub, core), self.ids[ident], target)

    def step1(self):
        self.push(0, self.up1, self.own1, self.own2)
        self.push(1, self.down1, self.own1, self.own2)

    def step2(self):
        before, after, _ = self.near1
        self.pull(0, self.up1, before, self.own2)
        self.push(2, self.up1, before, self.own2, 0)
        self.pull(1, self.down1, after, self.own2)
        self.push(3, self.down1, after, self.own2, 1)

    def step3(self):
        across = self.near1[2]
        self.pull(2, self.up1, across, self.own2, 0)
        self.pull(3, self.down1, across, self.own2, 1)
        self.push(4, self.up2, ALL, self.own2)
        self.push(5, self.down2, ALL, self.own2)
        self.share(8, self.own2)

    def step4(self):
        before, after, _ = self.near2
        self.pull(4, self.up2, ALL, before)
        self.push(6, self.up2, ALL, before, 0)
        self.pull(5, self.down2, ALL, after)
        self.push(7, self.down2, ALL, after, 1)
        self.share(9, before)
        self.share(10, after)

    def step5(self):
        across = self.near2[2]
        self.pull(6, self.up2, ALL, across, 0)
        self.pull(7, self.down2, ALL, across, 1)
        self.share(11, across)

    def step6(self):
        for place, ident in zip([self.own2] + self.near2, (8, 9, 10, 11)):
            self.pull(ident, self.sister, ALL, place, None, 1 - self.core)


def layer_kernel(
    total, res_h, q_h, kv_h, sink_ref, ow_h, g1_ref, b1_ref, up_h, dn_h, g2_ref, b2_ref, out_ref,
    qv, kvv, att, attr, resv, oww, upw, dnw, rows, act, pre, part, own, rin, rfin, bias, scores, weights, scale,
    local, send, recv, asend, arecv,
):
    sp, x = lax.axis_index("sp"), lax.axis_index("tp")
    core, chip = sp % 2, sp // 2
    y, z = chip % 4, chip // 4

    def device(zi, yi, ci, xi):
        return {"sp": ((zi % 4) * 4 + yi % 4) * 2 + ci, "tp": xi % 4}

    sister = device(z, y, 1 - core, x)
    right, left, across = (device(z, y, core, x + d) for d in (1, 3, 2))
    yup, ydown = device(z, y + 1, core, x), device(z, y + 3, core, x)
    zup, zdown = device(z + 1, y, core, x), device(z + 3, y, core, x)
    later, earlier = {"sp": (sp + 1) % 32, "tp": x}, {"sp": (sp + 31) % 32, "tp": x}

    loads = []

    def load(src, dst):
        copy = pltpu.make_async_copy(src, dst, local.at[len(loads)])
        copy.start()
        loads.append(copy)
        return copy

    kv_copy = load(kv_h, kvv.at[:, pl.ds(WINDOW, 1024), :])
    q_copy = load(q_h, qv)
    ow_copy = load(ow_h, oww.at[0])
    up_copy = load(up_h, upw.at[z, y, core])
    dn_copy = load(dn_h, dnw.at[z, y, core])
    res_copy = load(res_h, resv)

    barrier = pltpu.get_barrier_semaphore()
    far = {"sp": (sp + 31 + 2 * core) % 32, "tp": x}
    friends = (sister, right, left, across, yup, ydown, zup, zdown, far)
    for friend in friends:
        pl.semaphore_signal(barrier, inc=1, device_id=friend, device_id_type=MESH)
    with jax.named_scope("barrier"):
        pl.semaphore_wait(barrier, len(friends))

    links = Links(send, recv)
    halo = [links.take() for _ in range(2)]
    links.start(
        kv_h.at[:, pl.ds(1024 - WINDOW, WINDOW), :], kvv.at[:, pl.ds(0, WINDOW), :], halo[0], later
    )
    links.start(
        kv_h.at[:, pl.ds(0, WINDOW), :], kvv.at[:, pl.ds(1024 + WINDOW, WINDOW), :], halo[1], earlier
    )

    seed = [links.take() for _ in range(3)]
    seeds = ((right, 3), (left, 1), (across, 2))
    body_cols = pl.ds(XPART, 2048 - XPART)
    for ident, (target, place) in zip(seed, seeds):
        src = ow_h.at[z, y, core, :, body_cols]
        links.start(src, oww.at[place, z, y, core, :, body_cols], ident, target)
    xids = [links.take() for _ in range(7)]

    def xpart(place, ci, zs=ALL):
        return oww.at[place, zs, :, ci, :, pl.ds(0, XPART)]

    def xstart():
        src = ow_h.at[:, :, core, :, pl.ds(0, XPART)]
        links.start(src, xpart(3, core), xids[0], right)
        links.start(src, xpart(1, core), xids[1], left)

    def xpass():
        links.arrived(xpart(3, core), xids[0], right)
        near = xpart(3, core, pl.ds(0, 2))
        again = lambda place, zs=ALL: lambda: xpart(place, core, zs)
        links.start(near, xpart(2, core, pl.ds(0, 2)), xids[2], right, again(3, pl.ds(0, 2)))
        links.arrived(xpart(1, core), xids[1], left)
        near = xpart(1, core, pl.ds(2, 2))
        links.start(near, xpart(2, core, pl.ds(2, 2)), xids[3], left, again(1, pl.ds(2, 2)))
        links.start(xpart(3, core), xpart(3, core), xids[4], sister, again(3))
        links.start(xpart(1, core), xpart(1, core), xids[5], sister, again(1))

    def xshare():
        links.arrived(xpart(2, core, pl.ds(0, 2)), xids[2], right)
        links.arrived(xpart(2, core, pl.ds(2, 2)), xids[3], left)
        links.start(xpart(2, core), xpart(2, core), xids[6], sister)

    def xdone():
        for place, ident in ((3, 4), (1, 5), (2, 6)):
            links.arrived(xpart(place, 1 - core), xids[ident], sister)

    xstart()

    def ow_part(half, flip):
        def part_at(one, two, ci, sub):
            zi, yi = (two, one) if flip else (one, two)
            wide = (2048 - XPART) // 2
            at = XPART + half * wide
            if sub is not None:
                wide = wide // 2
                at = at + sub * wide
            return oww.at[pl.ds(1, 3), zi, yi, ci, :, pl.ds(at, wide)]

        return part_at

    def wide_part(buffer):
        def make(half, flip):
            def part_at(one, two, ci, sub):
                zi, yi = (two, one) if flip else (one, two)
                span = pl.ds(0, 64) if sub is None else pl.ds(sub * 32, 32)
                return buffer.at[zi, yi, ci, span, pl.ds(half * 1024, 1024)]

            return part_at

        return make

    def spread(make):
        return (
            Spread(links, make(0, False), z, y, core, (zup, zdown, yup, ydown), sister),
            Spread(links, make(1, True), y, z, core, (yup, ydown, zup, zdown), sister),
        )

    outs, ups, downs = spread(ow_part), spread(wide_part(upw)), spread(wide_part(dnw))

    def run(name, pair, step):
        with jax.named_scope(f"{name}{step}"):
            for one in pair:
                getattr(one, f"step{step}")()

    def seeded():
        with jax.named_scope("seed"):
            for ident, (target, place) in zip(seed, seeds):
                links.arrived(oww.at[place, z, y, core, :, body_cols], ident, target)
        run("outs", outs, 1)

    seeded()
    up_copy.wait()
    dn_copy.wait()
    q_copy.wait()
    kv_copy.wait()
    span = BLOCK + 2 * WINDOW
    iota_r = lax.broadcasted_iota(jnp.int32, (BLOCK, span), 0)
    iota_c = lax.broadcasted_iota(jnp.int32, (BLOCK, span), 1)

    def block_copy(index, half, step, target):
        return pltpu.make_async_remote_copy(
            src_ref=att.at[index],
            dst_ref=attr.at[half, :, pl.ds(aligned(3 - step, 512), 512)],
            send_sem=asend.at[half, step],
            recv_sem=arecv.at[half, step],
            device_id=target,
            device_id_type=MESH,
        )

    events = {
        1: lambda: (run("outs", outs, 2), run("ups", ups, 1))[1],
        3: lambda: run("outs", outs, 3),
        4: xpass,
        5: lambda: (run("ups", ups, 2), run("downs", downs, 1))[1],
    }

    def attend(index, carry):
        half, step = index // 4, index % 4
        owner = (x + 1 + step) % 4
        block = 2 * owner + half

        @pl.when(block == 0)
        def _():
            links.arrived(kvv.at[:, pl.ds(0, WINDOW), :], halo[0], later)

        @pl.when(block == 7)
        def _():
            links.arrived(kvv.at[:, pl.ds(1024 + WINDOW, WINDOW), :], halo[1], earlier)

        begin = aligned(block, BLOCK)
        pos = iota_c + (sp * 1024 + block * BLOCK - WINDOW)
        gap = iota_c - iota_r
        valid = (gap >= 0) & (gap <= 2 * WINDOW) & (pos >= 0) & (pos < total)
        bias[...] = jnp.where(valid, 0.0, -jnp.inf)
        for kv in range(4):
            lanes = slice(kv * HEAD_DIM, (kv + 1) * HEAD_DIM)
            keys = kvv[0, pl.ds(begin, span), lanes]
            pair = [
                qv[pl.ds(begin, BLOCK), slice(h * HEAD_DIM, (h + 1) * HEAD_DIM)]
                for h in (2 * kv, 2 * kv + 1)
            ]
            query = jnp.concatenate(pair, axis=0) * jnp.asarray(HEAD_DIM ** (-0.5), BF16)
            scores[kv] = lax.dot_general(
                query, keys, (((1,), (1,)), ((), ())), preferred_element_type=F32
            )
        for head in range(8):
            rows_of = slice((head % 2) * BLOCK, (head % 2 + 1) * BLOCK)
            score = scores[head // 2, rows_of] + bias[...]
            sink = sink_ref[head]
            top = jnp.maximum(jnp.max(score, axis=-1, keepdims=True), sink)
            expd = jnp.exp(score - top)
            denom = jnp.sum(expd, axis=-1, keepdims=True) + jnp.exp(sink - top)
            weights[head // 2, rows_of] = expd.astype(BF16)
            scale[head // 2, rows_of] = jnp.broadcast_to(1.0 / denom, (BLOCK, HEAD_DIM))
        for kv in range(4):
            lanes = slice(kv * HEAD_DIM, (kv + 1) * HEAD_DIM)
            values = kvv[1, pl.ds(begin, span), lanes]
            mixed = jnp.dot(weights[kv], values, preferred_element_type=F32) * scale[kv]
            for sub in range(2):
                head = 2 * kv + sub
                att[index, :, head * HEAD_DIM : (head + 1) * HEAD_DIM] = mixed[
                    sub * BLOCK : (sub + 1) * BLOCK
                ].astype(BF16)

        @pl.when(step < 3)
        def _():
            block_copy(index, half, step, {"sp": sp, "tp": owner}).start()

        @pl.when(step == 3)
        def _():
            attr[half, :, 0:512] = att[index]

        for when, event in events.items():
            pl.when(index == when)(event)
        return carry

    with jax.named_scope("attend"):
        lax.fori_loop(0, 8, attend, 0)

    def peer(step):
        return (right, across, left)[step]

    gather = [[links.take() for _ in range(6)] for _ in range(2)]
    low, high = pl.ds(0, 64), pl.ds(64, 64)

    def project(_):
        for half in range(2):
            for step in range(3):
                block_copy(4 * half + step, half, step, peer(step)).wait_recv()

        def body(n, carry):
            cols = pl.ds(aligned(n, 256), 256)
            weight = oww[:, :, :, :, :, cols].reshape(2048, 256)
            term = jnp.dot(attr[...].reshape(256, 2048), weight, preferred_element_type=F32)
            pre[:, cols] = term + resv[:, cols].astype(F32)
            return carry

        lax.fori_loop(0, 8, body, 0, unroll=4)

    def norm_first(half):
        def norm(i, carry):
            some = pl.ds(aligned(i, 32), 32)
            there = pl.ds(pl.multiple_of(half * 128 + i * 32, 32), 32)
            rows[half, 0, some, :] = norm_rows(pre[there, :], g1_ref[...], b1_ref[...])
            return carry

        lax.fori_loop(0, 4, norm, 0)

    def offer(half):
        ids = gather[half]
        links.start(rows.at[half, 0, low], rows.at[half, 3, low], ids[0], right)
        links.start(rows.at[half, 0, high], rows.at[half, 1, high], ids[1], left)
        links.start(rows.at[half, 0, high], rows.at[half, 3, high], ids[2], right)
        links.start(rows.at[half, 0, low], rows.at[half, 1, low], ids[3], left)

    def pass_on(half):
        ids = gather[half]
        links.arrived(rows.at[half, 3, low], ids[0], right)
        links.start(rows.at[half, 3, low], rows.at[half, 2, low], ids[4], right)
        links.arrived(rows.at[half, 1, high], ids[1], left)
        links.start(rows.at[half, 1, high], rows.at[half, 2, high], ids[5], left)

    def gathered(half):
        ids = gather[half]
        links.arrived(rows.at[half, 3, high], ids[2], right)
        links.arrived(rows.at[half, 1, low], ids[3], left)
        links.arrived(rows.at[half, 2, low], ids[4], right)
        links.arrived(rows.at[half, 2, high], ids[5], left)

    def up_project(half):
        def body(n, carry):
            cols = pl.ds(aligned(n, 256), 256)
            weight = upw[:, :, :, :, cols].reshape(2048, 256)
            hidden = jnp.dot(
                rows[half].reshape(512, 2048), weight, preferred_element_type=F32
            )
            act[:, cols] = jnp.square(jnp.maximum(hidden, 0.0)).astype(BF16)
            return carry

        lax.fori_loop(0, 8, body, 0, unroll=4)

    def scoped(name, phase, half):
        with jax.named_scope(f"{name}{half}"):
            phase(half)

    scatter = [[links.take() for _ in range(6)] for _ in range(2)]

    def down_project(half):
        def product(n, some):
            weight = dnw[n // 2, pl.ds((n % 2) * 2, 2)].reshape(256, 2048)
            return lax.dot_general(some, weight, (((1,), (1,)), ((), ())), preferred_element_type=F32)

        def body(n, carry):
            cols = pl.ds(aligned(n, 256), 256)
            term = product(n, act[128:384, :])
            part[half, 0, :, cols] = term[0:128].astype(BF16)
            part[half, 1, :, cols] = term[128:256].astype(BF16)
            return carry

        lax.fori_loop(0, 8, body, 0, unroll=4)
        ids = scatter[half]
        links.start(part.at[half, 1, low], rin.at[half, 0], ids[0], right)
        links.start(part.at[half, 1, high], rin.at[half, 1], ids[1], left)
        links.start(part.at[half, 0, high], rfin.at[half, 0, high], ids[2], right)

        def body(n, carry):
            cols = pl.ds(aligned(n, 256), 256)
            some = jnp.concatenate([act[384:512, :], act[0:128, :]], axis=0)
            term = product(n, some)
            part[half, 2, :, cols] = term[0:128].astype(BF16)
            own[half, :, cols] = term[128:256]
            return carry

        lax.fori_loop(0, 8, body, 0, unroll=4)
        links.start(part.at[half, 2, low], rfin.at[half, 1, low], ids[3], left)

    def join(half):
        ids = scatter[half]
        for side, (target, index, at) in enumerate(((right, 0, 0), (left, 2, 64))):
            links.arrived(rin.at[half, side], ids[side], target)
            span = pl.ds(at, 64)
            part[half, index, span, :] = (
                part[half, index, span, :].astype(F32) + rin[half, side].astype(F32)
            ).astype(BF16)
            links.start(
                part.at[half, index, span], rfin.at[half, side, span], ids[4 + side], target
            )

    def final(half):
        ids = scatter[half]
        links.arrived(rfin.at[half, 0, high], ids[2], right)
        links.arrived(rfin.at[half, 1, low], ids[3], left)
        links.arrived(rfin.at[half, 0, low], ids[4], right)
        links.arrived(rfin.at[half, 1, high], ids[5], left)

        def norm(i, carry):
            some = pl.ds(aligned(i, 32), 32)
            value = rows[half, 0, some, :].astype(F32) + own[half, some, :]
            value = value + rfin[half, 0, some, :].astype(F32)
            value = value + rfin[half, 1, some, :].astype(F32)
            there = pl.ds(pl.multiple_of(half * 128 + i * 32, 32), 32)
            out_ref[there, :] = norm_rows(value, g2_ref[...], b2_ref[...])
            return carry

        lax.fori_loop(0, 4, norm, 0)

    run("outs", outs, 4)
    with jax.named_scope("xshare"):
        xshare()
    run("downs", downs, 2)
    run("outs", outs, 5)
    run("ups", ups, 3)
    run("outs", outs, 6)
    with jax.named_scope("xdone"):
        xdone()
    ow_copy.wait()
    res_copy.wait()
    scoped("project", project, 0)
    scoped("norm_first", norm_first, 0)
    offer(0)
    scoped("norm_first", norm_first, 1)
    run("ups", ups, 4)
    run("downs", downs, 3)
    scoped("pass_on", pass_on, 0)
    offer(1)
    run("ups", ups, 5)
    run("ups", ups, 6)
    scoped("gathered", gathered, 0)
    scoped("up_project", up_project, 0)
    run("downs", downs, 4)
    scoped("pass_on", pass_on, 1)
    run("downs", downs, 5)
    run("downs", downs, 6)
    scoped("down_project", down_project, 0)
    scoped("gathered", gathered, 1)
    scoped("up_project", up_project, 1)
    scoped("join", join, 0)
    scoped("down_project", down_project, 1)
    scoped("final", final, 0)
    scoped("join", join, 1)
    for half in range(2):
        for step in range(3):
            block_copy(4 * half + step, half, step, peer(step)).wait_send()
    links.finish(2)
    scoped("final", final, 1)
    links.finish()


def on_device(res, q, kv, sink, ow, g1, b1, up, dn, g2, b2):
    total = q.shape[0] * lax.axis_size("sp")
    hbm = pl.BlockSpec(memory_space=pltpu.HBM)
    vmem = pl.BlockSpec(memory_space=pltpu.VMEM)
    smem = pl.BlockSpec(memory_space=pltpu.SMEM)
    return pl.pallas_call(
        functools.partial(layer_kernel, total),
        in_specs=[hbm, hbm, hbm, smem, hbm, vmem, vmem, hbm, hbm, vmem, vmem],
        out_specs=vmem,
        out_shape=pltpu.VMEM((256, 2048), BF16),
        scratch_shapes=[
            pltpu.VMEM((1024, 512), BF16),
            pltpu.VMEM((2, 1024 + 2 * WINDOW, 256), BF16),
            pltpu.VMEM((8, 128, 512), BF16),
            pltpu.VMEM((2, 128, 2048), BF16),
            pltpu.VMEM((256, 2048), BF16),
            pltpu.VMEM((4, 4, 4, 2, 16, 2048), BF16),
            pltpu.VMEM((4, 4, 2, 64, 2048), BF16),
            pltpu.VMEM((4, 4, 2, 64, 2048), BF16),
            pltpu.VMEM((2, 4, 128, 2048), BF16),
            pltpu.VMEM((512, 2048), BF16),
            pltpu.VMEM((256, 2048), F32),
            pltpu.VMEM((2, 3, 128, 2048), BF16),
            pltpu.VMEM((2, 128, 2048), F32),
            pltpu.VMEM((2, 2, 64, 2048), BF16),
            pltpu.VMEM((2, 2, 128, 2048), BF16),
            pltpu.VMEM((BLOCK, BLOCK + 2 * WINDOW), F32),
            pltpu.VMEM((4, 2 * BLOCK, BLOCK + 2 * WINDOW), F32),
            pltpu.VMEM((4, 2 * BLOCK, BLOCK + 2 * WINDOW), BF16),
            pltpu.VMEM((4, 2 * BLOCK, HEAD_DIM), F32),
            pltpu.SemaphoreType.DMA((8,)),
            pltpu.SemaphoreType.DMA((128,)),
            pltpu.SemaphoreType.DMA((128,)),
            pltpu.SemaphoreType.DMA((2, 3)),
            pltpu.SemaphoreType.DMA((2, 3)),
        ],
        compiler_params=pltpu.CompilerParams(
            collective_id=0, has_side_effects=True, vmem_limit_bytes=62 * 2**20
        ),
        cost_estimate=pl.CostEstimate(
            flops=2 * 10**10, bytes_accessed=24 * 2**20, transcendentals=4 * 10**6
        ),
        name="layer",
    )(
        res, q, kv, sink, ow.reshape(4, 4, 2, 16, 2048), g1.reshape(1, -1), b1.reshape(1, -1),
        up, dn.T, g2.reshape(1, -1), b2.reshape(1, -1),
    )


def solution(mesh):
    return jax.shard_map(
        on_device,
        mesh=mesh,
        in_specs=(
            P(("sp", "tp"), None),
            P("sp", "tp"),
            P(None, "sp", "tp"),
            P("tp"),
            P("tp", None),
            P(),
            P(),
            P("sp", "tp"),
            P("tp", "sp"),
            P(),
            P(),
        ),
        out_specs=P(("sp", "tp"), None),
        check_vma=False,
    )
```

```python
import functools

import jax
import jax.numpy as jnp
from jax import lax
from jax.experimental import pallas as pl
from jax.experimental.pallas import tpu as pltpu
from jax.sharding import PartitionSpec as P

HEAD_DIM = 64
WINDOW = 128
BLOCK = 128
XPART = 512
MESH = pl.DeviceIdType.MESH
F32 = jnp.float32
BF16 = jnp.bfloat16
ALL = slice(None)


def norm_rows(values, gain, bias):
    mean = jnp.mean(values, axis=-1, keepdims=True)
    centred = values - mean
    variance = jnp.mean(centred * centred, axis=-1, keepdims=True)
    return (centred * lax.rsqrt(variance + 1e-06) * gain + bias).astype(BF16)


def aligned(index, size):
    return pl.multiple_of(index * size, size)


class Links:
    def __init__(self, send, recv):
        self.send, self.recv, self.count, self.started = send, recv, 0, []

    def take(self):
        self.count += 1
        return self.count - 1

    def copy(self, src, dst, ident, target):
        return pltpu.make_async_remote_copy(
            src_ref=src,
            dst_ref=dst,
            send_sem=self.send.at[ident],
            recv_sem=self.recv.at[ident],
            device_id=target,
            device_id_type=MESH,
        )

    def start(self, src, dst, ident, target, again=None):
        self.copy(src, dst, ident, target).start()
        self.started.append((again or (lambda: src), ident, target))

    def arrived(self, dst, ident, target):
        self.copy(dst, dst, ident, target).wait_recv()

    def finish(self, keep=0):
        count = len(self.started) - keep
        for again, ident, target in self.started[:count]:
            src = again()
            self.copy(src, src, ident, target).wait_send()
        self.started = self.started[count:]


class Spread:
    def __init__(self, links, part, first, second, core, peers, sister, opposite=None):
        self.links, self.part, self.core, self.sister = links, part, core, sister
        self.opposite = opposite
        self.own1, self.own2 = first, second
        self.up1, self.down1, self.up2, self.down2 = peers
        self.ids = [links.take() for _ in range(14)]
        self.near1 = [(first + hop) % 4 for hop in (3, 1, 2)]
        self.near2 = [(second + hop) % 4 for hop in (3, 1, 2)]

    def at(self, one, two, sub=None, core=None):
        return self.part(one, two, self.core if core is None else core, sub)

    def push(self, ident, target, one, two, sub=None):
        place = self.at(one, two, sub)
        self.links.start(place, place, self.ids[ident], target, lambda: self.at(one, two, sub))

    def share(self, ident, two):
        for one in range(4):
            place = self.at(one, two)
            self.links.copy(place, place, self.ids[ident], self.sister).start()
        self.links.started.append((lambda: self.at(ALL, two), self.ids[ident], self.sister))

    def pull(self, ident, target, one, two, sub=None, core=None):
        self.links.arrived(self.at(one, two, sub, core), self.ids[ident], target)

    def step1(self):
        self.push(0, self.up1, self.own1, self.own2)
        self.push(1, self.down1, self.own1, self.own2)
        if self.opposite is not None:
            self.push(2, self.opposite, self.own1, self.own2)

    def step2(self):
        before, after, across = self.near1
        if self.opposite is not None:
            self.pull(0, self.up1, before, self.own2)
            self.pull(1, self.down1, after, self.own2)
            self.pull(2, self.opposite, across, self.own2)
            return
        self.pull(0, self.up1, before, self.own2)
        self.push(2, self.up1, before, self.own2, 0)
        self.pull(1, self.down1, after, self.own2)
        self.push(3, self.down1, after, self.own2, 1)

    def step3(self):
        across = self.near1[2]
        if self.opposite is None:
            self.pull(2, self.up1, across, self.own2, 0)
            self.pull(3, self.down1, across, self.own2, 1)
        self.push(4, self.up2, ALL, self.own2, 0)
        self.push(5, self.down2, ALL, self.own2, 1)
        self.push(12, self.up2, ALL, self.own2, 1)
        self.push(13, self.down2, ALL, self.own2, 0)
        self.share(8, self.own2)

    def step4(self):
        before, after, _ = self.near2
        self.pull(4, self.up2, ALL, before, 0)
        self.push(6, self.up2, ALL, before, 0)
        self.pull(5, self.down2, ALL, after, 1)
        self.push(7, self.down2, ALL, after, 1)

    def step5(self):
        before, after, _ = self.near2
        self.pull(12, self.up2, ALL, before, 1)
        self.share(9, before)
        self.pull(13, self.down2, ALL, after, 0)
        self.share(10, after)

    def step6(self):
        across = self.near2[2]
        self.pull(6, self.up2, ALL, across, 0)
        self.pull(7, self.down2, ALL, across, 1)
        self.share(11, across)

    def step7(self):
        for place, ident in zip([self.own2] + self.near2, (8, 9, 10, 11)):
            self.pull(ident, self.sister, ALL, place, None, 1 - self.core)


def layer_kernel(
    total, res_h, q_h, kv_h, sink_ref, ow_h, g1_ref, b1_ref, up_h, dn_h, g2_ref, b2_ref, out_ref,
    qv, kvv, att, attr, resv, oww, upw, dnw, rows, act, pre, part, own, rin, rfin, bias, scores, weights, scale,
    local, send, recv, asend, arecv,
):
    sp, x = lax.axis_index("sp"), lax.axis_index("tp")
    core, chip = sp % 2, sp // 2
    y, z = chip % 4, chip // 4

    def device(zi, yi, ci, xi):
        return {"sp": ((zi % 4) * 4 + yi % 4) * 2 + ci, "tp": xi % 4}

    sister = device(z, y, 1 - core, x)
    right, left, across = (device(z, y, core, x + d) for d in (1, 3, 2))
    yup, ydown = device(z, y + 1, core, x), device(z, y + 3, core, x)
    zup, zdown = device(z + 1, y, core, x), device(z + 3, y, core, x)
    later, earlier = {"sp": (sp + 1) % 32, "tp": x}, {"sp": (sp + 31) % 32, "tp": x}

    loads = []

    def load(src, dst):
        copy = pltpu.make_async_copy(src, dst, local.at[len(loads)])
        copy.start()
        loads.append(copy)
        return copy

    ow_copy = load(ow_h, oww.at[0])
    kv_copy = load(kv_h, kvv.at[:, pl.ds(WINDOW, 1024), :])
    q_copy = load(q_h, qv)
    up_copy = load(up_h, upw.at[z, y, core])
    dn_copy = load(dn_h, dnw.at[z, y, core])
    res_copy = load(res_h, resv)

    barrier = pltpu.get_barrier_semaphore()
    far = {"sp": (sp + 31 + 2 * core) % 32, "tp": x}
    zfar, yfar = device(z + 2, y, core, x), device(z, y + 2, core, x)
    friends = (sister, right, left, across, yup, ydown, zup, zdown, far, zfar, yfar)
    for friend in friends:
        pl.semaphore_signal(barrier, inc=1, device_id=friend, device_id_type=MESH)
    with jax.named_scope("barrier"):
        pl.semaphore_wait(barrier, len(friends))

    links = Links(send, recv)
    halo = [links.take() for _ in range(2)]

    seed = [links.take() for _ in range(3)]
    seeds = ((right, 3), (left, 1), (across, 2))
    body_cols = pl.ds(XPART, 2048 - XPART)
    ow_copy.wait()
    for ident, (target, place) in zip(seed, seeds):
        src = oww.at[0, z, y, core, :, body_cols]
        links.start(src, oww.at[place, z, y, core, :, body_cols], ident, target)
    xids = [links.take() for _ in range(7)]

    def xpart(place, ci, zs=ALL):
        return oww.at[place, zs, :, ci, :, pl.ds(0, XPART)]

    def xstart():
        src = xpart(0, core)
        links.start(src, xpart(3, core), xids[0], right)
        links.start(src, xpart(1, core), xids[1], left)

    def xpass():
        links.arrived(xpart(3, core), xids[0], right)
        near = xpart(3, core, pl.ds(0, 2))
        again = lambda place, zs=ALL: lambda: xpart(place, core, zs)
        links.start(near, xpart(2, core, pl.ds(0, 2)), xids[2], right, again(3, pl.ds(0, 2)))
        links.arrived(xpart(1, core), xids[1], left)
        near = xpart(1, core, pl.ds(2, 2))
        links.start(near, xpart(2, core, pl.ds(2, 2)), xids[3], left, again(1, pl.ds(2, 2)))
        links.start(xpart(3, core), xpart(3, core), xids[4], sister, again(3))
        links.start(xpart(1, core), xpart(1, core), xids[5], sister, again(1))

    def xshare():
        links.arrived(xpart(2, core, pl.ds(0, 2)), xids[2], right)
        links.arrived(xpart(2, core, pl.ds(2, 2)), xids[3], left)
        links.start(xpart(2, core), xpart(2, core), xids[6], sister)

    def xdone():
        for place, ident in ((3, 4), (1, 5), (2, 6)):
            links.arrived(xpart(place, 1 - core), xids[ident], sister)

    kv_copy.wait()
    last, start = pl.ds(1024, WINDOW), pl.ds(WINDOW, WINDOW)
    links.start(kvv.at[:, last, :], kvv.at[:, pl.ds(0, WINDOW), :], halo[0], later)
    links.start(kvv.at[:, start, :], kvv.at[:, pl.ds(1024 + WINDOW, WINDOW), :], halo[1], earlier)
    xstart()

    def ow_part(half, flip):
        def part_at(one, two, ci, sub):
            zi, yi = (two, one) if flip else (one, two)
            wide = (2048 - XPART) // 2
            at = XPART + half * wide
            if sub is not None:
                first = (wide + 128) // 256 * 128
                at, wide = at + sub * first, wide - first if sub else first
            return oww.at[pl.ds(1, 3), zi, yi, ci, :, pl.ds(at, wide)]

        return part_at

    def wide_part(buffer):
        def make(half, flip):
            def part_at(one, two, ci, sub):
                zi, yi = (two, one) if flip else (one, two)
                span = pl.ds(0, 64) if sub is None else pl.ds(sub * 32, 32)
                return buffer.at[zi, yi, ci, span, pl.ds(half * 1024, 1024)]

            return part_at

        return make

    def spread(make, zfar=None, yfar=None):
        return (
            Spread(links, make(0, False), z, y, core, (zup, zdown, yup, ydown), sister, zfar),
            Spread(links, make(1, True), y, z, core, (yup, ydown, zup, zdown), sister, yfar),
        )

    outs, ups, downs = spread(ow_part, zfar, yfar), spread(wide_part(upw)), spread(wide_part(dnw))

    def run(name, pair, step):
        with jax.named_scope(f"{name}{step}"):
            for one in pair:
                getattr(one, f"step{step}")()

    def seeded():
        with jax.named_scope("seed"):
            for ident, (target, place) in zip(seed, seeds):
                links.arrived(oww.at[place, z, y, core, :, body_cols], ident, target)
        run("outs", outs, 1)

    seeded()
    up_copy.wait()
    dn_copy.wait()
    q_copy.wait()
    span = BLOCK + 2 * WINDOW
    iota_r = lax.broadcasted_iota(jnp.int32, (BLOCK, span), 0)
    iota_c = lax.broadcasted_iota(jnp.int32, (BLOCK, span), 1)

    def block_copy(index, half, step, target):
        return pltpu.make_async_remote_copy(
            src_ref=att.at[index],
            dst_ref=attr.at[half, :, pl.ds(aligned(3 - step, 512), 512)],
            send_sem=asend.at[half, step],
            recv_sem=arecv.at[half, step],
            device_id=target,
            device_id_type=MESH,
        )

    events = {
        1: lambda: (run("outs", outs, 2), run("outs", outs, 3), run("ups", ups, 1))[2],
        4: xpass,
    }

    def attend(index, carry):
        half, step = index // 4, index % 4
        owner = (x + 1 + step) % 4
        block = 2 * owner + half

        @pl.when(block == 0)
        def _():
            links.arrived(kvv.at[:, pl.ds(0, WINDOW), :], halo[0], later)

        @pl.when(block == 7)
        def _():
            links.arrived(kvv.at[:, pl.ds(1024 + WINDOW, WINDOW), :], halo[1], earlier)

        begin = aligned(block, BLOCK)
        pos = iota_c + (sp * 1024 + block * BLOCK - WINDOW)
        gap = iota_c - iota_r
        valid = (gap >= 0) & (gap <= 2 * WINDOW) & (pos >= 0) & (pos < total)
        bias[...] = jnp.where(valid, 0.0, -jnp.inf)
        for kv in range(4):
            lanes = slice(kv * HEAD_DIM, (kv + 1) * HEAD_DIM)
            keys = kvv[0, pl.ds(begin, span), lanes]
            pair = [
                qv[pl.ds(begin, BLOCK), slice(h * HEAD_DIM, (h + 1) * HEAD_DIM)]
                for h in (2 * kv, 2 * kv + 1)
            ]
            query = jnp.concatenate(pair, axis=0) * jnp.asarray(HEAD_DIM ** (-0.5), BF16)
            scores[kv] = lax.dot_general(
                query, keys, (((1,), (1,)), ((), ())), preferred_element_type=F32
            )
        for head in range(8):
            rows_of = slice((head % 2) * BLOCK, (head % 2 + 1) * BLOCK)
            score = scores[head // 2, rows_of] + bias[...]
            sink = sink_ref[head]
            top = jnp.maximum(jnp.max(score, axis=-1, keepdims=True), sink)
            expd = jnp.exp(score - top)
            denom = jnp.sum(expd, axis=-1, keepdims=True) + jnp.exp(sink - top)
            weights[head // 2, rows_of] = expd.astype(BF16)
            scale[head // 2, rows_of] = jnp.broadcast_to(1.0 / denom, (BLOCK, HEAD_DIM))
        for kv in range(4):
            lanes = slice(kv * HEAD_DIM, (kv + 1) * HEAD_DIM)
            values = kvv[1, pl.ds(begin, span), lanes]
            mixed = jnp.dot(weights[kv], values, preferred_element_type=F32) * scale[kv]
            for sub in range(2):
                head = 2 * kv + sub
                att[index, :, head * HEAD_DIM : (head + 1) * HEAD_DIM] = mixed[
                    sub * BLOCK : (sub + 1) * BLOCK
                ].astype(BF16)

        @pl.when(step < 3)
        def _():
            block_copy(index, half, step, {"sp": sp, "tp": owner}).start()

        @pl.when(step == 3)
        def _():
            attr[half, :, 0:512] = att[index]

        for when, event in events.items():
            pl.when(index == when)(event)
        return carry

    with jax.named_scope("attend"):
        lax.fori_loop(0, 8, attend, 0)

    def peer(step):
        return (right, across, left)[step]

    gather = [[links.take() for _ in range(6)] for _ in range(2)]
    low, high = pl.ds(0, 64), pl.ds(64, 64)

    def project(_):
        for half in range(2):
            for step in range(3):
                block_copy(4 * half + step, half, step, peer(step)).wait_recv()

        def body(n, carry):
            cols = pl.ds(aligned(n, 256), 256)
            weight = oww[:, :, :, :, :, cols].reshape(2048, 256)
            term = jnp.dot(attr[...].reshape(256, 2048), weight, preferred_element_type=F32)
            pre[:, cols] = term + resv[:, cols].astype(F32)
            return carry

        lax.fori_loop(0, 8, body, 0, unroll=4)

    def norm_first(half):
        def norm(i, carry):
            some = pl.ds(aligned(i, 32), 32)
            there = pl.ds(pl.multiple_of(half * 128 + i * 32, 32), 32)
            rows[half, 0, some, :] = norm_rows(pre[there, :], g1_ref[...], b1_ref[...])
            return carry

        lax.fori_loop(0, 4, norm, 0)

    def offer(half):
        ids = gather[half]
        links.start(rows.at[half, 0, low], rows.at[half, 3, low], ids[0], right)
        links.start(rows.at[half, 0, high], rows.at[half, 1, high], ids[1], left)
        links.start(rows.at[half, 0, high], rows.at[half, 3, high], ids[2], right)
        links.start(rows.at[half, 0, low], rows.at[half, 1, low], ids[3], left)

    def pass_on(half):
        ids = gather[half]
        links.arrived(rows.at[half, 3, low], ids[0], right)
        links.start(rows.at[half, 3, low], rows.at[half, 2, low], ids[4], right)
        links.arrived(rows.at[half, 1, high], ids[1], left)
        links.start(rows.at[half, 1, high], rows.at[half, 2, high], ids[5], left)

    def gathered(half):
        ids = gather[half]
        links.arrived(rows.at[half, 3, high], ids[2], right)
        links.arrived(rows.at[half, 1, low], ids[3], left)
        links.arrived(rows.at[half, 2, low], ids[4], right)
        links.arrived(rows.at[half, 2, high], ids[5], left)

    def up_project(half):
        def body(n, carry):
            cols = pl.ds(aligned(n, 256), 256)
            weight = upw[:, :, :, :, cols].reshape(2048, 256)
            hidden = jnp.dot(
                rows[half].reshape(512, 2048), weight, preferred_element_type=F32
            )
            act[:, cols] = jnp.square(jnp.maximum(hidden, 0.0)).astype(BF16)
            return carry

        lax.fori_loop(0, 8, body, 0, unroll=4)

    def scoped(name, phase, half):
        with jax.named_scope(f"{name}{half}"):
            phase(half)

    scatter = [[links.take() for _ in range(6)] for _ in range(2)]

    def down_project(half):
        def product(n, some):
            weight = dnw[n // 2, pl.ds((n % 2) * 2, 2)].reshape(256, 2048)
            return lax.dot_general(some, weight, (((1,), (1,)), ((), ())), preferred_element_type=F32)

        def body(n, carry):
            cols = pl.ds(aligned(n, 256), 256)
            term = product(n, act[128:384, :])
            part[half, 0, :, cols] = term[0:128].astype(BF16)
            part[half, 1, :, cols] = term[128:256].astype(BF16)
            return carry

        lax.fori_loop(0, 8, body, 0, unroll=4)
        ids = scatter[half]
        links.start(part.at[half, 1, low], rin.at[half, 0], ids[0], right)
        links.start(part.at[half, 1, high], rin.at[half, 1], ids[1], left)
        links.start(part.at[half, 0, high], rfin.at[half, 0, high], ids[2], right)

        def body(n, carry):
            cols = pl.ds(aligned(n, 256), 256)
            some = jnp.concatenate([act[384:512, :], act[0:128, :]], axis=0)
            term = product(n, some)
            part[half, 2, :, cols] = term[0:128].astype(BF16)
            own[half, :, cols] = term[128:256]
            return carry

        lax.fori_loop(0, 8, body, 0, unroll=4)
        links.start(part.at[half, 2, low], rfin.at[half, 1, low], ids[3], left)

    def join(half):
        ids = scatter[half]
        for side, (target, index, at) in enumerate(((right, 0, 0), (left, 2, 64))):
            links.arrived(rin.at[half, side], ids[side], target)
            span = pl.ds(at, 64)
            part[half, index, span, :] = (
                part[half, index, span, :].astype(F32) + rin[half, side].astype(F32)
            ).astype(BF16)
            links.start(
                part.at[half, index, span], rfin.at[half, side, span], ids[4 + side], target
            )

    def final(half):
        ids = scatter[half]
        links.arrived(rfin.at[half, 0, high], ids[2], right)
        links.arrived(rfin.at[half, 1, low], ids[3], left)
        links.arrived(rfin.at[half, 0, low], ids[4], right)
        links.arrived(rfin.at[half, 1, high], ids[5], left)

        def norm(i, carry):
            some = pl.ds(aligned(i, 32), 32)
            value = rows[half, 0, some, :].astype(F32) + own[half, some, :]
            value = value + rfin[half, 0, some, :].astype(F32)
            value = value + rfin[half, 1, some, :].astype(F32)
            there = pl.ds(pl.multiple_of(half * 128 + i * 32, 32), 32)
            out_ref[there, :] = norm_rows(value, g2_ref[...], b2_ref[...])
            return carry

        lax.fori_loop(0, 4, norm, 0)

    run("outs", outs, 4)
    run("ups", ups, 2)
    run("downs", downs, 1)
    with jax.named_scope("xshare"):
        xshare()
    run("outs", outs, 5)
    run("outs", outs, 6)
    run("ups", ups, 3)
    run("outs", outs, 7)
    with jax.named_scope("xdone"):
        xdone()
    res_copy.wait()
    scoped("project", project, 0)
    scoped("norm_first", norm_first, 0)
    offer(0)
    scoped("norm_first", norm_first, 1)
    run("downs", downs, 2)
    run("ups", ups, 4)
    scoped("pass_on", pass_on, 0)
    offer(1)
    run("ups", ups, 5)
    run("downs", downs, 3)
    run("ups", ups, 6)
    run("ups", ups, 7)
    scoped("gathered", gathered, 0)
    run("downs", downs, 4)
    scoped("up_project", up_project, 0)
    run("downs", downs, 5)
    scoped("pass_on", pass_on, 1)
    run("downs", downs, 6)
    run("downs", downs, 7)
    scoped("down_project", down_project, 0)
    scoped("gathered", gathered, 1)
    scoped("up_project", up_project, 1)
    scoped("join", join, 0)
    scoped("down_project", down_project, 1)
    scoped("final", final, 0)
    scoped("join", join, 1)
    for half in range(2):
        for step in range(3):
            block_copy(4 * half + step, half, step, peer(step)).wait_send()
    links.finish(2)
    scoped("final", final, 1)
    links.finish()


def on_device(res, q, kv, sink, ow, g1, b1, up, dn, g2, b2):
    total = q.shape[0] * lax.axis_size("sp")
    hbm = pl.BlockSpec(memory_space=pltpu.HBM)
    vmem = pl.BlockSpec(memory_space=pltpu.VMEM)
    smem = pl.BlockSpec(memory_space=pltpu.SMEM)
    return pl.pallas_call(
        functools.partial(layer_kernel, total),
        in_specs=[hbm, hbm, hbm, smem, hbm, vmem, vmem, hbm, hbm, vmem, vmem],
        out_specs=vmem,
        out_shape=pltpu.VMEM((256, 2048), BF16),
        scratch_shapes=[
            pltpu.VMEM((1024, 512), BF16),
            pltpu.VMEM((2, 1024 + 2 * WINDOW, 256), BF16),
            pltpu.VMEM((8, 128, 512), BF16),
            pltpu.VMEM((2, 128, 2048), BF16),
            pltpu.VMEM((256, 2048), BF16),
            pltpu.VMEM((4, 4, 4, 2, 16, 2048), BF16),
            pltpu.VMEM((4, 4, 2, 64, 2048), BF16),
            pltpu.VMEM((4, 4, 2, 64, 2048), BF16),
            pltpu.VMEM((2, 4, 128, 2048), BF16),
            pltpu.VMEM((512, 2048), BF16),
            pltpu.VMEM((256, 2048), F32),
            pltpu.VMEM((2, 3, 128, 2048), BF16),
            pltpu.VMEM((2, 128, 2048), F32),
            pltpu.VMEM((2, 2, 64, 2048), BF16),
            pltpu.VMEM((2, 2, 128, 2048), BF16),
            pltpu.VMEM((BLOCK, BLOCK + 2 * WINDOW), F32),
            pltpu.VMEM((4, 2 * BLOCK, BLOCK + 2 * WINDOW), F32),
            pltpu.VMEM((4, 2 * BLOCK, BLOCK + 2 * WINDOW), BF16),
            pltpu.VMEM((4, 2 * BLOCK, HEAD_DIM), F32),
            pltpu.SemaphoreType.DMA((8,)),
            pltpu.SemaphoreType.DMA((128,)),
            pltpu.SemaphoreType.DMA((128,)),
            pltpu.SemaphoreType.DMA((2, 3)),
            pltpu.SemaphoreType.DMA((2, 3)),
        ],
        compiler_params=pltpu.CompilerParams(
            collective_id=0, has_side_effects=True, vmem_limit_bytes=62 * 2**20
        ),
        cost_estimate=pl.CostEstimate(
            flops=2 * 10**10, bytes_accessed=24 * 2**20, transcendentals=4 * 10**6
        ),
        name="layer",
    )(
        res, q, kv, sink, ow.reshape(4, 4, 2, 16, 2048), g1.reshape(1, -1), b1.reshape(1, -1),
        up, dn.T, g2.reshape(1, -1), b2.reshape(1, -1),
    )


def solution(mesh):
    return jax.shard_map(
        on_device,
        mesh=mesh,
        in_specs=(
            P(("sp", "tp"), None),
            P("sp", "tp"),
            P(None, "sp", "tp"),
            P("tp"),
            P("tp", None),
            P(),
            P(),
            P("sp", "tp"),
            P("tp", "sp"),
            P(),
            P(),
        ),
        out_specs=P(("sp", "tp"), None),
        check_vma=False,
    )
```

```python
import functools

import jax
import jax.numpy as jnp
from jax import lax
from jax.experimental import pallas as pl
from jax.experimental.pallas import tpu as pltpu
from jax.sharding import PartitionSpec as P

HEAD_DIM = 64
WINDOW = 128
BLOCK = 128
XPART = 768
SENDS = 40
MESH = pl.DeviceIdType.MESH
F32 = jnp.float32
BF16 = jnp.bfloat16
ALL = slice(None)


def norm_rows(values, gain, bias):
    mean = jnp.mean(values, axis=-1, keepdims=True)
    centred = values - mean
    variance = jnp.mean(centred * centred, axis=-1, keepdims=True)
    return (centred * lax.rsqrt(variance + 1e-06) * gain + bias).astype(BF16)


def aligned(index, size):
    return pl.multiple_of(index * size, size)


class Links:
    def __init__(self, send, recv):
        self.send, self.recv, self.count, self.started = send, recv, 0, []
        self.turn = 0

    def take(self):
        self.count += 1
        return self.count - 1

    def copy(self, src, dst, ident, target, slot=0):
        return pltpu.make_async_remote_copy(
            src_ref=src,
            dst_ref=dst,
            send_sem=self.send.at[slot],
            recv_sem=self.recv.at[ident],
            device_id=target,
            device_id_type=MESH,
        )

    def slot(self):
        slot = self.turn % SENDS
        self.turn += 1
        if self.turn > SENDS:
            self.left(self.started.pop(0))
        return slot

    def left(self, entry):
        again, ident, target, slot = entry
        src = again()
        self.copy(src, src, ident, target, slot).wait_send()

    def start(self, src, dst, ident, target, again=None):
        slot = self.slot()
        self.copy(src, dst, ident, target, slot).start()
        self.started.append((again or (lambda: src), ident, target, slot))

    def arrived(self, dst, ident, target):
        self.copy(dst, dst, ident, target).wait_recv()

    def finish(self, keep=0):
        while len(self.started) > keep:
            self.left(self.started.pop(0))


class Spread:
    def __init__(self, links, part, first, second, core, peers, sister, common, opposite=None):
        self.links, self.part, self.core, self.sister = links, part, core, sister
        self.opposite, self.common = opposite, common
        self.own1, self.own2 = first, second
        self.up1, self.down1, self.up2, self.down2 = peers
        self.ids = [links.take() for _ in range(10)]
        self.near1 = [(first + hop) % 4 for hop in (3, 1, 2)]
        self.near2 = [(second + hop) % 4 for hop in (3, 1, 2)]

    def at(self, one, two, sub=None, core=None):
        return self.part(one, two, self.core if core is None else core, sub)

    def push(self, ident, target, one, two, sub=None):
        place = self.at(one, two, sub)
        self.links.start(place, place, self.ids[ident], target, lambda: self.at(one, two, sub))

    def share(self, two, sub=None, far=False):
        slot, ident = self.links.slot(), self.common[far]
        for one in range(4):
            place = self.at(one, two, sub)
            self.links.copy(place, place, ident, self.sister, slot).start()
        entry = (lambda: self.at(ALL, two, sub), ident, self.sister, slot)
        self.links.started.append(entry)

    def pull(self, ident, target, one, two, sub=None, core=None):
        self.links.arrived(self.at(one, two, sub, core), self.ids[ident], target)

    def step1(self):
        self.push(0, self.up1, self.own1, self.own2)
        self.push(1, self.down1, self.own1, self.own2)
        if self.opposite is not None:
            self.push(2, self.opposite, self.own1, self.own2)

    def step2(self):
        before, after, across = self.near1
        if self.opposite is not None:
            self.pull(0, self.up1, before, self.own2)
            self.pull(1, self.down1, after, self.own2)
            self.pull(2, self.opposite, across, self.own2)
            return
        self.pull(0, self.up1, before, self.own2)
        self.push(2, self.up1, before, self.own2, 0)
        self.pull(1, self.down1, after, self.own2)
        self.push(3, self.down1, after, self.own2, 1)

    def step3(self):
        across = self.near1[2]
        if self.opposite is None:
            self.pull(2, self.up1, across, self.own2, 0)
            self.pull(3, self.down1, across, self.own2, 1)
        self.push(4, self.up2, ALL, self.own2, 0)
        self.push(5, self.down2, ALL, self.own2, 1)
        self.push(8, self.up2, ALL, self.own2, 1)
        self.push(9, self.down2, ALL, self.own2, 0)
        self.share(self.own2)

    def step4(self):
        before, after, _ = self.near2
        self.pull(4, self.up2, ALL, before, 0)
        self.push(6, self.up2, ALL, before, 0)
        self.pull(5, self.down2, ALL, after, 1)
        self.push(7, self.down2, ALL, after, 1)
        self.share(before, 0)
        self.share(after, 1)

    def step5(self):
        before, after, _ = self.near2
        self.pull(8, self.up2, ALL, before, 1)
        self.share(before, 1)
        self.pull(9, self.down2, ALL, after, 0)
        self.share(after, 0)

    def step6(self):
        across = self.near2[2]
        self.pull(6, self.up2, ALL, across, 0)
        self.pull(7, self.down2, ALL, across, 1)
        self.share(across, far=True)


def layer_kernel(
    total, res_h, q_h, kv_h, sink_h, ow_h, g1_h, b1_h, up_h, dn_h, g2_h, b2_h, out_ref,
    qv, kvv, att, attr, resv, oww, upw, dnw, rows, act, pre, part, own, rin, rfin, bias, scores, weights, scale,
    sink_ref, g1_ref, b1_ref, g2_ref, b2_ref, local, send, recv, asend, arecv,
):
    sp, x = lax.axis_index("sp"), lax.axis_index("tp")
    core, chip = sp % 2, sp // 2
    y, z = chip % 4, chip // 4

    def device(zi, yi, ci, xi):
        return {"sp": ((zi % 4) * 4 + yi % 4) * 2 + ci, "tp": xi % 4}

    sister = device(z, y, 1 - core, x)
    right, left, across = (device(z, y, core, x + d) for d in (1, 3, 2))
    yup, ydown = device(z, y + 1, core, x), device(z, y + 3, core, x)
    zup, zdown = device(z + 1, y, core, x), device(z + 3, y, core, x)
    later, earlier = {"sp": (sp + 1) % 32, "tp": x}, {"sp": (sp + 31) % 32, "tp": x}

    loads = []

    def load(src, dst):
        copy = pltpu.make_async_copy(src, dst, local.at[len(loads)])
        copy.start()
        loads.append(copy)
        return copy

    ow_copy = load(ow_h, oww.at[0])
    kv_copy = load(kv_h, kvv.at[:, pl.ds(WINDOW, 1024), :])
    q_copy = load(q_h, qv)
    up_copy = load(up_h, upw.at[z, y, core])
    dn_copy = load(dn_h, dnw.at[z, y, core])
    sink_copy = load(sink_h, sink_ref)
    res_copy = load(res_h, resv)
    pairs = ((g1_h, g1_ref), (b1_h, b1_ref), (g2_h, g2_ref), (b2_h, b2_ref))
    norm_copies = [load(src, dst) for src, dst in pairs]

    barrier = pltpu.get_barrier_semaphore()
    far = {"sp": (sp + 31 + 2 * core) % 32, "tp": x}
    zfar, yfar = device(z + 2, y, core, x), device(z, y + 2, core, x)
    friends = (sister, right, left, across, yup, ydown, zup, zdown, far, zfar, yfar)
    for friend in friends:
        pl.semaphore_signal(barrier, inc=1, device_id=friend, device_id_type=MESH)
    with jax.named_scope("barrier"):
        pl.semaphore_wait(barrier, len(friends))

    links = Links(send, recv)
    halo = [links.take() for _ in range(2)]

    seed = links.take()
    seeds = ((right, 3), (left, 1), (across, 2))
    body_cols = pl.ds(XPART, 2048 - XPART)
    ow_copy.wait()
    for target, place in seeds:
        src = oww.at[0, z, y, core, :, body_cols]
        links.start(src, oww.at[place, z, y, core, :, body_cols], seed, target)
    xids = [links.take() for _ in range(4)]

    def xpart(place, ci, zs=ALL):
        return oww.at[place, zs, :, ci, :, pl.ds(0, XPART)]

    def xstart():
        src = xpart(0, core)
        links.start(src, xpart(3, core), xids[0], right)
        links.start(src, xpart(1, core), xids[1], left)

    def xpass():
        links.arrived(xpart(3, core), xids[0], right)
        near = xpart(3, core, pl.ds(0, 2))
        again = lambda place, zs=ALL: lambda: xpart(place, core, zs)
        links.start(near, xpart(2, core, pl.ds(0, 2)), xids[2], right, again(3, pl.ds(0, 2)))
        links.arrived(xpart(1, core), xids[1], left)
        near = xpart(1, core, pl.ds(2, 2))
        links.start(near, xpart(2, core, pl.ds(2, 2)), xids[3], left, again(1, pl.ds(2, 2)))
        links.start(xpart(3, core), xpart(3, core), ow_all, sister, again(3))
        links.start(xpart(1, core), xpart(1, core), ow_all, sister, again(1))

    def xshare():
        links.arrived(xpart(2, core, pl.ds(0, 2)), xids[2], right)
        links.arrived(xpart(2, core, pl.ds(2, 2)), xids[3], left)
        links.start(xpart(2, core), xpart(2, core), ow_all, sister)

    kv_copy.wait()
    last, start = pl.ds(1024, WINDOW), pl.ds(WINDOW, WINDOW)
    links.start(kvv.at[:, last, :], kvv.at[:, pl.ds(0, WINDOW), :], halo[0], later)
    links.start(kvv.at[:, start, :], kvv.at[:, pl.ds(1024 + WINDOW, WINDOW), :], halo[1], earlier)
    xstart()

    def ow_part(half, flip):
        def part_at(one, two, ci, sub):
            zi, yi = (two, one) if flip else (one, two)
            wide = (2048 - XPART) // 2
            at = XPART + half * wide
            if sub is not None:
                first = (wide + 128) // 256 * 128
                at, wide = at + sub * first, wide - first if sub else first
            return oww.at[pl.ds(1, 3), zi, yi, ci, :, pl.ds(at, wide)]

        return part_at

    def wide_part(buffer):
        def make(half, flip):
            def part_at(one, two, ci, sub):
                zi, yi = (two, one) if flip else (one, two)
                span = pl.ds(0, 64) if sub is None else pl.ds(sub * 32, 32)
                return buffer.at[zi, yi, ci, span, pl.ds(half * 1024, 1024)]

            return part_at

        return make

    def spread(make, common, zfar=None, yfar=None):
        return (
            Spread(links, make(0, False), z, y, core, (zup, zdown, yup, ydown), sister, common, zfar),
            Spread(links, make(1, True), y, z, core, (yup, ydown, zup, zdown), sister, common, yfar),
        )

    ow_all, up_all, dn_near, dn_far = (links.take() for _ in range(4))
    outs = spread(ow_part, (ow_all, ow_all), zfar, yfar)
    ups = spread(wide_part(upw), (up_all, up_all))
    downs = spread(wide_part(dnw), (dn_near, dn_far))

    def run(name, pair, step):
        with jax.named_scope(f"{name}{step}"):
            for one in pair:
                getattr(one, f"step{step}")()

    def seeded():
        with jax.named_scope("seed"):
            links.arrived(oww.at[pl.ds(1, 3), z, y, core, :, body_cols], seed, right)
        run("outs", outs, 1)

    def complete(name, half, ident):
        with jax.named_scope(f"{name}7"):
            links.arrived(half, ident, sister)

    up_copy.wait()
    run("ups", ups, 1)
    dn_copy.wait()
    seeded()
    q_copy.wait()
    sink_copy.wait()
    span = BLOCK + 2 * WINDOW
    iota_r = lax.broadcasted_iota(jnp.int32, (BLOCK, span), 0)
    iota_c = lax.broadcasted_iota(jnp.int32, (BLOCK, span), 1)

    def block_copy(index, half, step, target):
        return pltpu.make_async_remote_copy(
            src_ref=att.at[index],
            dst_ref=attr.at[half, :, pl.ds(aligned(3 - step, 512), 512)],
            send_sem=asend.at[half, step],
            recv_sem=arecv.at[half, step],
            device_id=target,
            device_id_type=MESH,
        )

    events = {
        1: lambda: (run("outs", outs, 2), run("outs", outs, 3), run("ups", ups, 2))[2],
        3: lambda: run("downs", downs, 1),
        4: xpass,
        6: lambda: run("outs", outs, 4),
    }

    def attend(index, carry):
        half, step = index // 4, index % 4
        owner = (x + 1 + step) % 4
        block = 2 * owner + half

        @pl.when(block == 0)
        def _():
            links.arrived(kvv.at[:, pl.ds(0, WINDOW), :], halo[0], later)

        @pl.when(block == 7)
        def _():
            links.arrived(kvv.at[:, pl.ds(1024 + WINDOW, WINDOW), :], halo[1], earlier)

        begin = aligned(block, BLOCK)
        pos = iota_c + (sp * 1024 + block * BLOCK - WINDOW)
        gap = iota_c - iota_r
        valid = (gap >= 0) & (gap <= 2 * WINDOW) & (pos >= 0) & (pos < total)
        bias[...] = jnp.where(valid, 0.0, -jnp.inf)
        for kv in range(4):
            lanes = slice(kv * HEAD_DIM, (kv + 1) * HEAD_DIM)
            keys = kvv[0, pl.ds(begin, span), lanes]
            pair = [
                qv[pl.ds(begin, BLOCK), slice(h * HEAD_DIM, (h + 1) * HEAD_DIM)]
                for h in (2 * kv, 2 * kv + 1)
            ]
            query = jnp.concatenate(pair, axis=0) * jnp.asarray(HEAD_DIM ** (-0.5), BF16)
            scores[kv] = lax.dot_general(
                query, keys, (((1,), (1,)), ((), ())), preferred_element_type=F32
            )
        for head in range(8):
            rows_of = slice((head % 2) * BLOCK, (head % 2 + 1) * BLOCK)
            score = scores[head // 2, rows_of] + bias[...]
            sink = sink_ref[head]
            top = jnp.maximum(jnp.max(score, axis=-1, keepdims=True), sink)
            expd = jnp.exp(score - top)
            denom = jnp.sum(expd, axis=-1, keepdims=True) + jnp.exp(sink - top)
            weights[head // 2, rows_of] = expd.astype(BF16)
            scale[head // 2, rows_of] = jnp.broadcast_to(1.0 / denom, (BLOCK, HEAD_DIM))
        for kv in range(4):
            lanes = slice(kv * HEAD_DIM, (kv + 1) * HEAD_DIM)
            values = kvv[1, pl.ds(begin, span), lanes]
            mixed = jnp.dot(weights[kv], values, preferred_element_type=F32) * scale[kv]
            for sub in range(2):
                head = 2 * kv + sub
                att[index, :, head * HEAD_DIM : (head + 1) * HEAD_DIM] = mixed[
                    sub * BLOCK : (sub + 1) * BLOCK
                ].astype(BF16)

        @pl.when(step < 3)
        def _():
            block_copy(index, half, step, {"sp": sp, "tp": owner}).start()

        @pl.when(step == 3)
        def _():
            attr[half, :, 0:512] = att[index]

        for when, event in events.items():
            pl.when(index == when)(event)
        return carry

    with jax.named_scope("attend"):
        lax.fori_loop(0, 8, attend, 0)

    def peer(step):
        return (right, across, left)[step]

    gather = [[links.take() for _ in range(3)] for _ in range(2)]
    low, high = pl.ds(0, 64), pl.ds(64, 64)

    def project(half):
        for step in range(3):
            block_copy(4 * half + step, half, step, peer(step)).wait_recv()

        def body(n, carry):
            cols = pl.ds(aligned(n, 256), 256)
            weight = oww[:, :, :, :, :, cols].reshape(2048, 256)
            term = jnp.dot(attr[half], weight, preferred_element_type=F32)
            there = slice(half * 128, half * 128 + 128)
            pre[there, cols] = term + resv[there, cols].astype(F32)
            return carry

        lax.fori_loop(0, 8, body, 0, unroll=4)

    def norm_first(half):
        def norm(i, carry):
            some = pl.ds(aligned(i, 32), 32)
            there = pl.ds(pl.multiple_of(half * 128 + i * 32, 32), 32)
            rows[half, 0, some, :] = norm_rows(pre[there, :], g1_ref[...], b1_ref[...])
            return carry

        lax.fori_loop(0, 4, norm, 0)

    def offer(half):
        ids = gather[half]
        links.start(rows.at[half, 0, low], rows.at[half, 3, low], ids[0], right)
        links.start(rows.at[half, 0, high], rows.at[half, 1, high], ids[1], left)
        links.start(rows.at[half, 0, high], rows.at[half, 3, high], ids[2], right)
        links.start(rows.at[half, 0, low], rows.at[half, 1, low], ids[2], left)

    def pass_on(half):
        ids = gather[half]
        links.arrived(rows.at[half, 3, low], ids[0], right)
        links.start(rows.at[half, 3, low], rows.at[half, 2, low], ids[2], right)
        links.arrived(rows.at[half, 1, high], ids[1], left)
        links.start(rows.at[half, 1, high], rows.at[half, 2, high], ids[2], left)

    def gathered(half):
        links.arrived(rows.at[half, pl.ds(1, 2)], gather[half][2], right)

    def up_project(half):
        def body(n, carry):
            cols = pl.ds(aligned(n, 256), 256)
            weight = upw[:, :, :, :, cols].reshape(2048, 256)
            hidden = jnp.dot(
                rows[half].reshape(512, 2048), weight, preferred_element_type=F32
            )
            act[:, cols] = jnp.square(jnp.maximum(hidden, 0.0)).astype(BF16)
            return carry

        lax.fori_loop(0, 8, body, 0, unroll=4)

    def scoped(name, phase, half):
        with jax.named_scope(f"{name}{half}"):
            phase(half)

    scatter = [[links.take() for _ in range(3)] for _ in range(2)]

    def down_project(half):
        def product(n, some):
            weight = dnw[n // 2, pl.ds((n % 2) * 2, 2)].reshape(256, 2048)
            return lax.dot_general(some, weight, (((1,), (1,)), ((), ())), preferred_element_type=F32)

        def body(n, carry):
            cols = pl.ds(aligned(n, 256), 256)
            term = product(n, act[128:384, :])
            part[half, 0, :, cols] = term[0:128].astype(BF16)
            part[half, 1, :, cols] = term[128:256].astype(BF16)
            return carry

        def tile(n):
            body(n, 0)

        if half:
            lax.fori_loop(0, 8, body, 0, unroll=4)
        else:
            there = (y + 2) % 4 // 2
            for hop in (0, 1, 3):
                tile((z + hop) % 4 * 2 + 1 - there)
            run("downs", downs, 6)
            complete("downs", dnw.at[0, :, 1 - core], dn_far)
            for hop in (0, 1, 3):
                tile((z + hop) % 4 * 2 + there)
            for pair in range(2):
                tile((z + 2) % 4 * 2 + pair)
        ids = scatter[half]
        links.start(part.at[half, 1, low], rin.at[half, 0], ids[0], right)
        links.start(part.at[half, 1, high], rin.at[half, 1], ids[1], left)
        links.start(part.at[half, 0, high], rfin.at[half, 0, high], ids[2], right)

        def body(n, carry):
            cols = pl.ds(aligned(n, 256), 256)
            some = jnp.concatenate([act[384:512, :], act[0:128, :]], axis=0)
            term = product(n, some)
            part[half, 2, :, cols] = term[0:128].astype(BF16)
            own[half, :, cols] = term[128:256]
            return carry

        lax.fori_loop(0, 8, body, 0, unroll=4)
        links.start(part.at[half, 2, low], rfin.at[half, 1, low], ids[2], left)

    def join(half):
        ids = scatter[half]
        for side, (target, index, at) in enumerate(((right, 0, 0), (left, 2, 64))):
            links.arrived(rin.at[half, side], ids[side], target)
            span = pl.ds(at, 64)
            part[half, index, span, :] = (
                part[half, index, span, :].astype(F32) + rin[half, side].astype(F32)
            ).astype(BF16)
            links.start(
                part.at[half, index, span], rfin.at[half, side, span], ids[2], target
            )

    def final(half):
        links.arrived(rfin.at[half], scatter[half][2], right)

        def norm(i, carry):
            some = pl.ds(aligned(i, 32), 32)
            value = rows[half, 0, some, :].astype(F32) + own[half, some, :]
            value = value + rfin[half, 0, some, :].astype(F32)
            value = value + rfin[half, 1, some, :].astype(F32)
            there = pl.ds(pl.multiple_of(half * 128 + i * 32, 32), 32)
            out_ref[there, :] = norm_rows(value, g2_ref[...], b2_ref[...])
            return carry

        lax.fori_loop(0, 4, norm, 0)

    run("outs", outs, 5)
    run("downs", downs, 2)
    run("ups", ups, 3)
    run("outs", outs, 6)
    with jax.named_scope("xshare"):
        xshare()
    complete("outs", oww.at[pl.ds(1, 3), :, :, 1 - core], ow_all)
    res_copy.wait()
    for copy in norm_copies:
        copy.wait()
    scoped("project", project, 0)
    scoped("norm_first", norm_first, 0)
    offer(0)
    scoped("project", project, 1)
    scoped("norm_first", norm_first, 1)
    run("ups", ups, 4)
    scoped("pass_on", pass_on, 0)
    offer(1)
    run("ups", ups, 5)
    run("downs", downs, 3)
    run("ups", ups, 6)
    complete("ups", upw.at[:, :, 1 - core], up_all)
    scoped("gathered", gathered, 0)
    run("downs", downs, 4)
    scoped("up_project", up_project, 0)
    run("downs", downs, 5)
    scoped("pass_on", pass_on, 1)
    complete("near", dnw.at[pl.ds(0, 3), :, 1 - core], dn_near)
    scoped("down_project", down_project, 0)
    scoped("gathered", gathered, 1)
    scoped("up_project", up_project, 1)
    scoped("join", join, 0)
    scoped("down_project", down_project, 1)
    scoped("final", final, 0)
    scoped("join", join, 1)
    for half in range(2):
        for step in range(3):
            block_copy(4 * half + step, half, step, peer(step)).wait_send()
    links.finish(2)
    scoped("final", final, 1)
    with jax.named_scope("finish"):
        links.finish()


def on_device(res, q, kv, sink, ow, g1, b1, up, dn, g2, b2):
    total = q.shape[0] * lax.axis_size("sp")
    hbm = pl.BlockSpec(memory_space=pltpu.HBM)
    vmem = pl.BlockSpec(memory_space=pltpu.VMEM)
    return pl.pallas_call(
        functools.partial(layer_kernel, total),
        in_specs=[hbm] * 11,
        out_specs=vmem,
        out_shape=pltpu.VMEM((256, 2048), BF16),
        scratch_shapes=[
            pltpu.VMEM((1024, 512), BF16),
            pltpu.VMEM((2, 1024 + 2 * WINDOW, 256), BF16),
            pltpu.VMEM((8, 128, 512), BF16),
            pltpu.VMEM((2, 128, 2048), BF16),
            pltpu.VMEM((256, 2048), BF16),
            pltpu.VMEM((4, 4, 4, 2, 16, 2048), BF16),
            pltpu.VMEM((4, 4, 2, 64, 2048), BF16),
            pltpu.VMEM((4, 4, 2, 64, 2048), BF16),
            pltpu.VMEM((2, 4, 128, 2048), BF16),
            pltpu.VMEM((512, 2048), BF16),
            pltpu.VMEM((256, 2048), F32),
            pltpu.VMEM((2, 3, 128, 2048), BF16),
            pltpu.VMEM((2, 128, 2048), F32),
            pltpu.VMEM((2, 2, 64, 2048), BF16),
            pltpu.VMEM((2, 2, 128, 2048), BF16),
            pltpu.VMEM((BLOCK, BLOCK + 2 * WINDOW), F32),
            pltpu.VMEM((4, 2 * BLOCK, BLOCK + 2 * WINDOW), F32),
            pltpu.VMEM((4, 2 * BLOCK, BLOCK + 2 * WINDOW), BF16),
            pltpu.VMEM((4, 2 * BLOCK, HEAD_DIM), F32),
            pltpu.SMEM((8,), F32),
            pltpu.VMEM((1, 2048), F32),
            pltpu.VMEM((1, 2048), F32),
            pltpu.VMEM((1, 2048), F32),
            pltpu.VMEM((1, 2048), F32),
            pltpu.SemaphoreType.DMA((12,)),
            pltpu.SemaphoreType.DMA((SENDS,)),
            pltpu.SemaphoreType.DMA((83,)),
            pltpu.SemaphoreType.DMA((2, 3)),
            pltpu.SemaphoreType.DMA((2, 3)),
        ],
        compiler_params=pltpu.CompilerParams(
            collective_id=0, has_side_effects=True, vmem_limit_bytes=62 * 2**20
        ),
        cost_estimate=pl.CostEstimate(
            flops=2 * 10**10, bytes_accessed=24 * 2**20, transcendentals=4 * 10**6
        ),
        name="layer",
    )(
        res, q, kv, sink, ow.reshape(4, 4, 2, 16, 2048), g1.reshape(1, -1), b1.reshape(1, -1),
        up, dn.T, g2.reshape(1, -1), b2.reshape(1, -1),
    )


def solution(mesh):
    return jax.shard_map(
        on_device,
        mesh=mesh,
        in_specs=(
            P(("sp", "tp"), None),
            P("sp", "tp"),
            P(None, "sp", "tp"),
            P("tp"),
            P("tp", None),
            P(),
            P(),
            P("sp", "tp"),
            P("tp", "sp"),
            P(),
            P(),
        ),
        out_specs=P(("sp", "tp"), None),
        check_vma=False,
    )
```

```python
import functools

import jax
import jax.numpy as jnp
from jax import lax
from jax.experimental import pallas as pl
from jax.experimental.pallas import tpu as pltpu
from jax.sharding import PartitionSpec as P

HEAD_DIM = 64
WINDOW = 128
BLOCK = 128
XPART = 768
SENDS = 40
MESH = pl.DeviceIdType.MESH
F32 = jnp.float32
BF16 = jnp.bfloat16
ALL = slice(None)


def norm_rows(values, gain, bias):
    mean = jnp.mean(values, axis=-1, keepdims=True)
    centred = values - mean
    variance = jnp.mean(centred * centred, axis=-1, keepdims=True)
    return (centred * lax.rsqrt(variance + 1e-06) * gain + bias).astype(BF16)


def aligned(index, size):
    return pl.multiple_of(index * size, size)


class Links:
    def __init__(self, send, recv):
        self.send, self.recv, self.count, self.started = send, recv, 0, []
        self.turn = 0

    def take(self):
        self.count += 1
        return self.count - 1

    def copy(self, src, dst, ident, target, slot=0):
        return pltpu.make_async_remote_copy(
            src_ref=src,
            dst_ref=dst,
            send_sem=self.send.at[slot],
            recv_sem=self.recv.at[ident],
            device_id=target,
            device_id_type=MESH,
        )

    def slot(self):
        slot = self.turn % SENDS
        self.turn += 1
        if self.turn > SENDS:
            self.left(self.started.pop(0))
        return slot

    def left(self, entry):
        again, ident, target, slot = entry
        src = again()
        self.copy(src, src, ident, target, slot).wait_send()

    def start(self, src, dst, ident, target, again=None):
        slot = self.slot()
        self.copy(src, dst, ident, target, slot).start()
        self.started.append((again or (lambda: src), ident, target, slot))

    def arrived(self, dst, ident, target):
        self.copy(dst, dst, ident, target).wait_recv()

    def finish(self, keep=0):
        while len(self.started) > keep:
            self.left(self.started.pop(0))


class Spread:
    def __init__(self, links, part, first, second, core, peers, sister, common, opposite=None):
        self.links, self.part, self.core, self.sister = links, part, core, sister
        self.opposite, self.common = opposite, common
        self.own1, self.own2 = first, second
        self.up1, self.down1, self.up2, self.down2 = peers
        self.ids = [links.take() for _ in range(10)]
        self.near1 = [(first + hop) % 4 for hop in (3, 1, 2)]
        self.near2 = [(second + hop) % 4 for hop in (3, 1, 2)]

    def at(self, one, two, sub=None, core=None):
        return self.part(one, two, self.core if core is None else core, sub)

    def push(self, ident, target, one, two, sub=None):
        place = self.at(one, two, sub)
        self.links.start(place, place, self.ids[ident], target, lambda: self.at(one, two, sub))

    def share(self, two, sub=None, far=False):
        slot, ident = self.links.slot(), self.common[far]
        for one in range(4):
            place = self.at(one, two, sub)
            self.links.copy(place, place, ident, self.sister, slot).start()
        entry = (lambda: self.at(ALL, two, sub), ident, self.sister, slot)
        self.links.started.append(entry)

    def pull(self, ident, target, one, two, sub=None, core=None):
        self.links.arrived(self.at(one, two, sub, core), self.ids[ident], target)

    def step1(self):
        self.push(0, self.up1, self.own1, self.own2)
        self.push(1, self.down1, self.own1, self.own2)
        if self.opposite is not None:
            self.push(2, self.opposite, self.own1, self.own2)

    def step2(self):
        before, after, across = self.near1
        if self.opposite is not None:
            self.pull(0, self.up1, before, self.own2)
            self.pull(1, self.down1, after, self.own2)
            self.pull(2, self.opposite, across, self.own2)
            return
        self.pull(0, self.up1, before, self.own2)
        self.push(2, self.up1, before, self.own2, 0)
        self.pull(1, self.down1, after, self.own2)
        self.push(3, self.down1, after, self.own2, 1)

    def step3(self):
        across = self.near1[2]
        if self.opposite is None:
            self.pull(2, self.up1, across, self.own2, 0)
            self.pull(3, self.down1, across, self.own2, 1)
        self.push(4, self.up2, ALL, self.own2, 0)
        self.push(5, self.down2, ALL, self.own2, 1)
        self.push(8, self.up2, ALL, self.own2, 1)
        self.push(9, self.down2, ALL, self.own2, 0)
        self.share(self.own2)

    def step4(self):
        before, after, _ = self.near2
        self.pull(4, self.up2, ALL, before, 0)
        self.push(6, self.up2, ALL, before, 0)
        self.pull(5, self.down2, ALL, after, 1)
        self.push(7, self.down2, ALL, after, 1)
        self.share(before, 0)
        self.share(after, 1)

    def step5(self):
        before, after, _ = self.near2
        self.pull(8, self.up2, ALL, before, 1)
        self.share(before, 1)
        self.pull(9, self.down2, ALL, after, 0)
        self.share(after, 0)

    def step6(self):
        across = self.near2[2]
        self.pull(6, self.up2, ALL, across, 0)
        self.pull(7, self.down2, ALL, across, 1)
        self.share(across, far=True)


def layer_kernel(
    total, res_h, q_h, kv_h, sink_h, ow_h, g1_h, b1_h, up_h, dn_h, g2_h, b2_h, out_ref,
    qv, kvv, att, attr, resv, oww, upw, dnw, rows, act, pre, part, own, rin, rfin, bias, scores, weights, scale,
    sink_ref, g1_ref, b1_ref, g2_ref, b2_ref, local, send, recv, asend, arecv,
):
    sp, x = lax.axis_index("sp"), lax.axis_index("tp")
    core, chip = sp % 2, sp // 2
    y, z = chip % 4, chip // 4

    def device(zi, yi, ci, xi):
        return {"sp": ((zi % 4) * 4 + yi % 4) * 2 + ci, "tp": xi % 4}

    sister = device(z, y, 1 - core, x)
    right, left, across = (device(z, y, core, x + d) for d in (1, 3, 2))
    yup, ydown = device(z, y + 1, core, x), device(z, y + 3, core, x)
    zup, zdown = device(z + 1, y, core, x), device(z + 3, y, core, x)
    later, earlier = {"sp": (sp + 1) % 32, "tp": x}, {"sp": (sp + 31) % 32, "tp": x}

    loads = []

    def load(src, dst):
        copy = pltpu.make_async_copy(src, dst, local.at[len(loads)])
        copy.start()
        loads.append(copy)
        return copy

    ow_copy = load(ow_h, oww.at[0])
    kv_copy = load(kv_h, kvv.at[:, pl.ds(WINDOW, 1024), :])
    q_copy = load(q_h, qv)
    up_copy = load(up_h, upw.at[z, y, core])
    dn_copy = load(dn_h, dnw.at[z, y, core])
    sink_copy = load(sink_h, sink_ref)
    res_copy = load(res_h, resv)
    pairs = ((g1_h, g1_ref), (b1_h, b1_ref), (g2_h, g2_ref), (b2_h, b2_ref))
    norm_copies = [load(src, dst) for src, dst in pairs]

    barrier = pltpu.get_barrier_semaphore()
    far = {"sp": (sp + 31 + 2 * core) % 32, "tp": x}
    zfar, yfar = device(z + 2, y, core, x), device(z, y + 2, core, x)
    friends = (sister, right, left, across, yup, ydown, zup, zdown, far, zfar, yfar)
    for friend in friends:
        pl.semaphore_signal(barrier, inc=1, device_id=friend, device_id_type=MESH)
    with jax.named_scope("barrier"):
        pl.semaphore_wait(barrier, len(friends))

    links = Links(send, recv)
    halo = [links.take() for _ in range(2)]

    seed = links.take()
    seeds = ((right, 3), (left, 1), (across, 2))
    body_cols = pl.ds(XPART, 2048 - XPART)
    ow_copy.wait()
    for target, place in seeds:
        src = oww.at[0, z, y, core, :, body_cols]
        links.start(src, oww.at[place, z, y, core, :, body_cols], seed, target)
    xids = [links.take() for _ in range(4)]

    def xpart(place, ci, zs=ALL):
        return oww.at[place, zs, :, ci, :, pl.ds(0, XPART)]

    def xstart():
        src = xpart(0, core)
        links.start(src, xpart(3, core), xids[0], right)
        links.start(src, xpart(1, core), xids[1], left)

    def xpass():
        links.arrived(xpart(3, core), xids[0], right)
        near = xpart(3, core, pl.ds(0, 2))
        again = lambda place, zs=ALL: lambda: xpart(place, core, zs)
        links.start(near, xpart(2, core, pl.ds(0, 2)), xids[2], right, again(3, pl.ds(0, 2)))
        links.arrived(xpart(1, core), xids[1], left)
        near = xpart(1, core, pl.ds(2, 2))
        links.start(near, xpart(2, core, pl.ds(2, 2)), xids[3], left, again(1, pl.ds(2, 2)))
        links.start(xpart(3, core), xpart(3, core), ow_all, sister, again(3))
        links.start(xpart(1, core), xpart(1, core), ow_all, sister, again(1))

    def xshare():
        links.arrived(xpart(2, core, pl.ds(0, 2)), xids[2], right)
        links.arrived(xpart(2, core, pl.ds(2, 2)), xids[3], left)
        links.start(xpart(2, core), xpart(2, core), ow_all, sister)

    kv_copy.wait()
    last, start = pl.ds(1024, WINDOW), pl.ds(WINDOW, WINDOW)
    links.start(kvv.at[:, last, :], kvv.at[:, pl.ds(0, WINDOW), :], halo[0], later)
    links.start(kvv.at[:, start, :], kvv.at[:, pl.ds(1024 + WINDOW, WINDOW), :], halo[1], earlier)
    xstart()

    def ow_part(half, flip):
        def part_at(one, two, ci, sub):
            zi, yi = (two, one) if flip else (one, two)
            wide = (2048 - XPART) // 2
            at = XPART + half * wide
            if sub is not None:
                first = (wide + 128) // 256 * 128
                at, wide = at + sub * first, wide - first if sub else first
            return oww.at[pl.ds(1, 3), zi, yi, ci, :, pl.ds(at, wide)]

        return part_at

    def wide_part(buffer):
        def make(half, flip):
            def part_at(one, two, ci, sub):
                zi, yi = (two, one) if flip else (one, two)
                span = pl.ds(0, 64) if sub is None else pl.ds(sub * 32, 32)
                return buffer.at[zi, yi, ci, span, pl.ds(half * 1024, 1024)]

            return part_at

        return make

    def spread(make, common, zfar=None, yfar=None):
        return (
            Spread(links, make(0, False), z, y, core, (zup, zdown, yup, ydown), sister, common, zfar),
            Spread(links, make(1, True), y, z, core, (yup, ydown, zup, zdown), sister, common, yfar),
        )

    ow_all, up_all, dn_near, dn_far = (links.take() for _ in range(4))
    outs = spread(ow_part, (ow_all, ow_all), zfar, yfar)
    ups = spread(wide_part(upw), (up_all, up_all))
    downs = spread(wide_part(dnw), (dn_near, dn_far))

    def run(name, pair, step):
        with jax.named_scope(f"{name}{step}"):
            for one in pair:
                getattr(one, f"step{step}")()

    def seeded():
        with jax.named_scope("seed"):
            links.arrived(oww.at[pl.ds(1, 3), z, y, core, :, body_cols], seed, right)
        run("outs", outs, 1)

    def complete(name, half, ident):
        with jax.named_scope(f"{name}7"):
            links.arrived(half, ident, sister)

    up_copy.wait()
    run("ups", ups, 1)
    dn_copy.wait()
    seeded()
    q_copy.wait()
    sink_copy.wait()
    span = BLOCK + 2 * WINDOW
    iota_r = lax.broadcasted_iota(jnp.int32, (BLOCK, span), 0)
    iota_c = lax.broadcasted_iota(jnp.int32, (BLOCK, span), 1)

    def block_copy(index, half, step, target):
        return pltpu.make_async_remote_copy(
            src_ref=att.at[index],
            dst_ref=attr.at[half, :, pl.ds(aligned(3 - step, 512), 512)],
            send_sem=asend.at[half, step],
            recv_sem=arecv.at[half, step],
            device_id=target,
            device_id_type=MESH,
        )

    events = {
        1: lambda: (run("outs", outs, 2), run("outs", outs, 3), run("ups", ups, 2))[2],
        3: xpass,
        5: lambda: (run("outs", outs, 4), run("downs", downs, 1))[1],
        6: lambda: run("ups", ups, 3),
    }

    def attend(index, carry):
        half, step = index // 4, index % 4
        owner = (x + 1 + step) % 4
        block = 2 * owner + half

        @pl.when(block == 0)
        def _():
            links.arrived(kvv.at[:, pl.ds(0, WINDOW), :], halo[0], later)

        @pl.when(block == 7)
        def _():
            links.arrived(kvv.at[:, pl.ds(1024 + WINDOW, WINDOW), :], halo[1], earlier)

        begin = aligned(block, BLOCK)
        pos = iota_c + (sp * 1024 + block * BLOCK - WINDOW)
        gap = iota_c - iota_r
        valid = (gap >= 0) & (gap <= 2 * WINDOW) & (pos >= 0) & (pos < total)
        bias[...] = jnp.where(valid, 0.0, -jnp.inf)
        for kv in range(4):
            lanes = slice(kv * HEAD_DIM, (kv + 1) * HEAD_DIM)
            keys = kvv[0, pl.ds(begin, span), lanes]
            pair = [
                qv[pl.ds(begin, BLOCK), slice(h * HEAD_DIM, (h + 1) * HEAD_DIM)]
                for h in (2 * kv, 2 * kv + 1)
            ]
            query = jnp.concatenate(pair, axis=0) * jnp.asarray(HEAD_DIM ** (-0.5), BF16)
            scores[kv] = lax.dot_general(
                query, keys, (((1,), (1,)), ((), ())), preferred_element_type=F32
            )
        for head in range(8):
            rows_of = slice((head % 2) * BLOCK, (head % 2 + 1) * BLOCK)
            score = scores[head // 2, rows_of] + bias[...]
            sink = sink_ref[head]
            top = jnp.maximum(jnp.max(score, axis=-1, keepdims=True), sink)
            expd = jnp.exp(score - top)
            denom = jnp.sum(expd, axis=-1, keepdims=True) + jnp.exp(sink - top)
            weights[head // 2, rows_of] = expd.astype(BF16)
            scale[head // 2, rows_of] = jnp.broadcast_to(1.0 / denom, (BLOCK, HEAD_DIM))
        for kv in range(4):
            lanes = slice(kv * HEAD_DIM, (kv + 1) * HEAD_DIM)
            values = kvv[1, pl.ds(begin, span), lanes]
            mixed = jnp.dot(weights[kv], values, preferred_element_type=F32) * scale[kv]
            for sub in range(2):
                head = 2 * kv + sub
                att[index, :, head * HEAD_DIM : (head + 1) * HEAD_DIM] = mixed[
                    sub * BLOCK : (sub + 1) * BLOCK
                ].astype(BF16)

        @pl.when(step < 3)
        def _():
            block_copy(index, half, step, {"sp": sp, "tp": owner}).start()

        @pl.when(step == 3)
        def _():
            attr[half, :, 0:512] = att[index]

        for when, event in events.items():
            pl.when(index == when)(event)
        return carry

    with jax.named_scope("attend"):
        lax.fori_loop(0, 8, attend, 0)

    def peer(step):
        return (right, across, left)[step]

    gather = [[links.take() for _ in range(3)] for _ in range(2)]
    low, high = pl.ds(0, 64), pl.ds(64, 64)

    def project(half):
        for step in range(3):
            block_copy(4 * half + step, half, step, peer(step)).wait_recv()

        def body(n, carry):
            cols = pl.ds(aligned(n, 256), 256)
            weight = oww[:, :, :, :, :, cols].reshape(2048, 256)
            term = jnp.dot(attr[half], weight, preferred_element_type=F32)
            there = slice(half * 128, half * 128 + 128)
            pre[there, cols] = term + resv[there, cols].astype(F32)
            return carry

        lax.fori_loop(0, 8, body, 0, unroll=4)

    def norm_first(half):
        def norm(i, carry):
            some = pl.ds(aligned(i, 32), 32)
            there = pl.ds(pl.multiple_of(half * 128 + i * 32, 32), 32)
            rows[half, 0, some, :] = norm_rows(pre[there, :], g1_ref[...], b1_ref[...])
            return carry

        lax.fori_loop(0, 4, norm, 0, unroll=2)

    def offer(half):
        ids = gather[half]
        links.start(rows.at[half, 0, low], rows.at[half, 3, low], ids[0], right)
        links.start(rows.at[half, 0, high], rows.at[half, 1, high], ids[1], left)
        links.start(rows.at[half, 0, high], rows.at[half, 3, high], ids[2], right)
        links.start(rows.at[half, 0, low], rows.at[half, 1, low], ids[2], left)

    def pass_on(half):
        ids = gather[half]
        links.arrived(rows.at[half, 3, low], ids[0], right)
        links.start(rows.at[half, 3, low], rows.at[half, 2, low], ids[2], right)
        links.arrived(rows.at[half, 1, high], ids[1], left)
        links.start(rows.at[half, 1, high], rows.at[half, 2, high], ids[2], left)

    def gathered(half):
        links.arrived(rows.at[half, pl.ds(1, 2)], gather[half][2], right)

    def up_project(half):
        def body(n, carry):
            cols = pl.ds(aligned(n, 256), 256)
            weight = upw[:, :, :, :, cols].reshape(2048, 256)
            hidden = jnp.dot(
                rows[half].reshape(512, 2048), weight, preferred_element_type=F32
            )
            act[:, cols] = jnp.square(jnp.maximum(hidden, 0.0)).astype(BF16)
            return carry

        lax.fori_loop(0, 8, body, 0, unroll=4)

    def scoped(name, phase, half):
        with jax.named_scope(f"{name}{half}"):
            phase(half)

    scatter = [[links.take() for _ in range(3)] for _ in range(2)]

    def down_project(half):
        def product(n, some):
            weight = dnw[n // 2, pl.ds((n % 2) * 2, 2)].reshape(256, 2048)
            return lax.dot_general(some, weight, (((1,), (1,)), ((), ())), preferred_element_type=F32)

        def body(n, carry):
            cols = pl.ds(aligned(n, 256), 256)
            term = product(n, act[128:384, :])
            part[half, 0, :, cols] = term[0:128].astype(BF16)
            part[half, 1, :, cols] = term[128:256].astype(BF16)
            return carry

        def tile(n):
            body(n, 0)

        if half:
            lax.fori_loop(0, 8, body, 0, unroll=4)
        else:
            there = (y + 2) % 4 // 2
            for hop in (0, 1, 3):
                tile((z + hop) % 4 * 2 + 1 - there)
            run("downs", downs, 6)
            complete("downs", dnw.at[0, :, 1 - core], dn_far)
            for hop in (0, 1, 3):
                tile((z + hop) % 4 * 2 + there)
            for pair in range(2):
                tile((z + 2) % 4 * 2 + pair)
        ids = scatter[half]
        links.start(part.at[half, 1, low], rin.at[half, 0], ids[0], right)
        links.start(part.at[half, 1, high], rin.at[half, 1], ids[1], left)
        links.start(part.at[half, 0, high], rfin.at[half, 0, high], ids[2], right)

        def body(n, carry):
            cols = pl.ds(aligned(n, 256), 256)
            some = jnp.concatenate([act[384:512, :], act[0:128, :]], axis=0)
            term = product(n, some)
            part[half, 2, :, cols] = term[0:128].astype(BF16)
            own[half, :, cols] = term[128:256]
            return carry

        lax.fori_loop(0, 8, body, 0, unroll=4)
        links.start(part.at[half, 2, low], rfin.at[half, 1, low], ids[2], left)

    def join(half):
        ids = scatter[half]
        for side, (target, index, at) in enumerate(((right, 0, 0), (left, 2, 64))):
            links.arrived(rin.at[half, side], ids[side], target)
            span = pl.ds(at, 64)
            part[half, index, span, :] = (
                part[half, index, span, :].astype(F32) + rin[half, side].astype(F32)
            ).astype(BF16)
            links.start(
                part.at[half, index, span], rfin.at[half, side, span], ids[2], target
            )

    def final(half):
        links.arrived(rfin.at[half], scatter[half][2], right)

        def norm(i, carry):
            some = pl.ds(aligned(i, 32), 32)
            value = rows[half, 0, some, :].astype(F32) + own[half, some, :]
            value = value + rfin[half, 0, some, :].astype(F32)
            value = value + rfin[half, 1, some, :].astype(F32)
            there = pl.ds(pl.multiple_of(half * 128 + i * 32, 32), 32)
            out_ref[there, :] = norm_rows(value, g2_ref[...], b2_ref[...])
            return carry

        lax.fori_loop(0, 4, norm, 0, unroll=2)

    run("outs", outs, 5)
    run("outs", outs, 6)
    with jax.named_scope("xshare"):
        xshare()
    complete("outs", oww.at[pl.ds(1, 3), :, :, 1 - core], ow_all)
    res_copy.wait()
    for copy in norm_copies:
        copy.wait()
    scoped("project", project, 0)
    scoped("norm_first", norm_first, 0)
    offer(0)
    scoped("project", project, 1)
    scoped("norm_first", norm_first, 1)
    run("downs", downs, 2)
    run("ups", ups, 4)
    scoped("pass_on", pass_on, 0)
    offer(1)
    run("ups", ups, 5)
    run("downs", downs, 3)
    run("ups", ups, 6)
    complete("ups", upw.at[:, :, 1 - core], up_all)
    scoped("gathered", gathered, 0)
    run("downs", downs, 4)
    scoped("up_project", up_project, 0)
    run("downs", downs, 5)
    scoped("pass_on", pass_on, 1)
    complete("near", dnw.at[pl.ds(0, 3), :, 1 - core], dn_near)
    scoped("down_project", down_project, 0)
    scoped("gathered", gathered, 1)
    scoped("up_project", up_project, 1)
    scoped("join", join, 0)
    scoped("down_project", down_project, 1)
    scoped("final", final, 0)
    scoped("join", join, 1)
    for half in range(2):
        for step in range(3):
            block_copy(4 * half + step, half, step, peer(step)).wait_send()
    links.finish(2)
    scoped("final", final, 1)
    with jax.named_scope("finish"):
        links.finish()


def on_device(res, q, kv, sink, ow, g1, b1, up, dn, g2, b2):
    total = q.shape[0] * lax.axis_size("sp")
    hbm = pl.BlockSpec(memory_space=pltpu.HBM)
    vmem = pl.BlockSpec(memory_space=pltpu.VMEM)
    return pl.pallas_call(
        functools.partial(layer_kernel, total),
        in_specs=[hbm] * 11,
        out_specs=vmem,
        out_shape=pltpu.VMEM((256, 2048), BF16),
        scratch_shapes=[
            pltpu.VMEM((1024, 512), BF16),
            pltpu.VMEM((2, 1024 + 2 * WINDOW, 256), BF16),
            pltpu.VMEM((8, 128, 512), BF16),
            pltpu.VMEM((2, 128, 2048), BF16),
            pltpu.VMEM((256, 2048), BF16),
            pltpu.VMEM((4, 4, 4, 2, 16, 2048), BF16),
            pltpu.VMEM((4, 4, 2, 64, 2048), BF16),
            pltpu.VMEM((4, 4, 2, 64, 2048), BF16),
            pltpu.VMEM((2, 4, 128, 2048), BF16),
            pltpu.VMEM((512, 2048), BF16),
            pltpu.VMEM((256, 2048), F32),
            pltpu.VMEM((2, 3, 128, 2048), BF16),
            pltpu.VMEM((2, 128, 2048), F32),
            pltpu.VMEM((2, 2, 64, 2048), BF16),
            pltpu.VMEM((2, 2, 128, 2048), BF16),
            pltpu.VMEM((BLOCK, BLOCK + 2 * WINDOW), F32),
            pltpu.VMEM((4, 2 * BLOCK, BLOCK + 2 * WINDOW), F32),
            pltpu.VMEM((4, 2 * BLOCK, BLOCK + 2 * WINDOW), BF16),
            pltpu.VMEM((4, 2 * BLOCK, HEAD_DIM), F32),
            pltpu.SMEM((8,), F32),
            pltpu.VMEM((1, 2048), F32),
            pltpu.VMEM((1, 2048), F32),
            pltpu.VMEM((1, 2048), F32),
            pltpu.VMEM((1, 2048), F32),
            pltpu.SemaphoreType.DMA((12,)),
            pltpu.SemaphoreType.DMA((SENDS,)),
            pltpu.SemaphoreType.DMA((83,)),
            pltpu.SemaphoreType.DMA((2, 3)),
            pltpu.SemaphoreType.DMA((2, 3)),
        ],
        compiler_params=pltpu.CompilerParams(
            collective_id=0, has_side_effects=True, vmem_limit_bytes=62 * 2**20
        ),
        cost_estimate=pl.CostEstimate(
            flops=2 * 10**10, bytes_accessed=24 * 2**20, transcendentals=4 * 10**6
        ),
        name="layer",
    )(
        res, q, kv, sink, ow.reshape(4, 4, 2, 16, 2048), g1.reshape(1, -1), b1.reshape(1, -1),
        up, dn.T, g2.reshape(1, -1), b2.reshape(1, -1),
    )


def solution(mesh):
    return jax.shard_map(
        on_device,
        mesh=mesh,
        in_specs=(
            P(("sp", "tp"), None),
            P("sp", "tp"),
            P(None, "sp", "tp"),
            P("tp"),
            P("tp", None),
            P(),
            P(),
            P("sp", "tp"),
            P("tp", "sp"),
            P(),
            P(),
        ),
        out_specs=P(("sp", "tp"), None),
        check_vma=False,
    )
```

```python
import functools

import jax
import jax.numpy as jnp
from jax import lax
from jax.experimental import pallas as pl
from jax.experimental.pallas import tpu as pltpu
from jax.sharding import PartitionSpec as P

HEAD_DIM = 64
WINDOW = 128
BLOCK = 128
XPART = 768
SENDS = 56
MESH = pl.DeviceIdType.MESH
F32 = jnp.float32
BF16 = jnp.bfloat16
ALL = slice(None)


def norm_rows(values, gain, bias):
    mean = jnp.mean(values, axis=-1, keepdims=True)
    centred = values - mean
    variance = jnp.mean(centred * centred, axis=-1, keepdims=True)
    return (centred * lax.rsqrt(variance + 1e-06) * gain + bias).astype(BF16)


def aligned(index, size):
    return pl.multiple_of(index * size, size)


class Links:
    def __init__(self, send, recv):
        self.send, self.recv, self.count, self.started = send, recv, 0, []
        self.turn = 0

    def take(self):
        self.count += 1
        return self.count - 1

    def copy(self, src, dst, ident, target, slot=0):
        return pltpu.make_async_remote_copy(
            src_ref=src,
            dst_ref=dst,
            send_sem=self.send.at[slot],
            recv_sem=self.recv.at[ident],
            device_id=target,
            device_id_type=MESH,
        )

    def slot(self):
        slot = self.turn % SENDS
        self.turn += 1
        if self.turn > SENDS:
            self.left(self.started.pop(0))
        return slot

    def left(self, entry):
        again, ident, target, slot = entry
        src = again()
        self.copy(src, src, ident, target, slot).wait_send()

    def start(self, src, dst, ident, target, again=None):
        slot = self.slot()
        self.copy(src, dst, ident, target, slot).start()
        self.started.append((again or (lambda: src), ident, target, slot))

    def arrived(self, dst, ident, target):
        self.copy(dst, dst, ident, target).wait_recv()

    def finish(self, keep=0):
        while len(self.started) > keep:
            self.left(self.started.pop(0))


class Spread:
    def __init__(self, links, part, first, second, core, peers, sister, common, opposite=None):
        self.links, self.part, self.core, self.sister = links, part, core, sister
        self.opposite, self.common = opposite, common
        self.own1, self.own2 = first, second
        self.up1, self.down1, self.up2, self.down2 = peers
        self.ids = [links.take() for _ in range(10)]
        self.near1 = [(first + hop) % 4 for hop in (3, 1, 2)]
        self.near2 = [(second + hop) % 4 for hop in (3, 1, 2)]

    def at(self, one, two, sub=None, core=None):
        return self.part(one, two, self.core if core is None else core, sub)

    def push(self, ident, target, one, two, sub=None):
        place = self.at(one, two, sub)
        self.links.start(place, place, self.ids[ident], target, lambda: self.at(one, two, sub))

    def share(self, two, sub=None, far=False):
        slot, ident = self.links.slot(), self.common[far]
        for one in range(4):
            place = self.at(one, two, sub)
            self.links.copy(place, place, ident, self.sister, slot).start()
        entry = (lambda: self.at(ALL, two, sub), ident, self.sister, slot)
        self.links.started.append(entry)

    def pull(self, ident, target, one, two, sub=None, core=None):
        self.links.arrived(self.at(one, two, sub, core), self.ids[ident], target)

    def step1(self):
        self.push(0, self.up1, self.own1, self.own2)
        self.push(1, self.down1, self.own1, self.own2)
        if self.opposite is not None:
            self.push(2, self.opposite, self.own1, self.own2)

    def step2(self):
        before, after, across = self.near1
        if self.opposite is not None:
            self.pull(0, self.up1, before, self.own2)
            self.pull(1, self.down1, after, self.own2)
            self.pull(2, self.opposite, across, self.own2)
            return
        self.pull(0, self.up1, before, self.own2)
        self.push(2, self.up1, before, self.own2, 0)
        self.pull(1, self.down1, after, self.own2)
        self.push(3, self.down1, after, self.own2, 1)

    def step3(self):
        across = self.near1[2]
        if self.opposite is None:
            self.pull(2, self.up1, across, self.own2, 0)
            self.pull(3, self.down1, across, self.own2, 1)
        self.push(4, self.up2, ALL, self.own2, 0)
        self.push(5, self.down2, ALL, self.own2, 1)
        self.push(8, self.up2, ALL, self.own2, 1)
        self.push(9, self.down2, ALL, self.own2, 0)
        self.share(self.own2)

    def step4(self):
        before, after, _ = self.near2
        self.pull(4, self.up2, ALL, before, 0)
        self.push(6, self.up2, ALL, before, 0)
        self.pull(5, self.down2, ALL, after, 1)
        self.push(7, self.down2, ALL, after, 1)
        self.share(before, 0)
        self.share(after, 1)

    def step5(self):
        before, after, _ = self.near2
        self.pull(8, self.up2, ALL, before, 1)
        self.share(before, 1)
        self.pull(9, self.down2, ALL, after, 0)
        self.share(after, 0)

    def step6(self):
        across = self.near2[2]
        self.pull(6, self.up2, ALL, across, 0)
        self.pull(7, self.down2, ALL, across, 1)
        self.share(across, far=True)


def layer_kernel(
    total, res_h, q_h, kv_h, sink_h, ow_h, g1_h, b1_h, up_h, dn_h, g2_h, b2_h, out_ref,
    qv, kvv, att, attr, resv, oww, upw, dnw, rows, act, pre, part, own, rin, rfin, bias, scores, weights, scale,
    sink_ref, g1_ref, b1_ref, g2_ref, b2_ref, local, send, recv, asend, arecv,
):
    sp, x = lax.axis_index("sp"), lax.axis_index("tp")
    core, chip = sp % 2, sp // 2
    y, z = chip % 4, chip // 4

    def device(zi, yi, ci, xi):
        return {"sp": ((zi % 4) * 4 + yi % 4) * 2 + ci, "tp": xi % 4}

    sister = device(z, y, 1 - core, x)
    right, left, across = (device(z, y, core, x + d) for d in (1, 3, 2))
    yup, ydown = device(z, y + 1, core, x), device(z, y + 3, core, x)
    zup, zdown = device(z + 1, y, core, x), device(z + 3, y, core, x)
    later, earlier = {"sp": (sp + 1) % 32, "tp": x}, {"sp": (sp + 31) % 32, "tp": x}

    loads = []

    def load(src, dst):
        copy = pltpu.make_async_copy(src, dst, local.at[len(loads)])
        copy.start()
        loads.append(copy)
        return copy

    ow_copy = load(ow_h, oww.at[0])
    kv_copy = load(kv_h, kvv.at[:, pl.ds(WINDOW, 1024), :])
    q_copy = load(q_h, qv)
    up_copy = load(up_h, upw.at[z, y, core])
    dn_copy = load(dn_h, dnw.at[z, y, core])
    sink_copy = load(sink_h, sink_ref)
    res_copy = load(res_h, resv)
    pairs = ((g1_h, g1_ref), (b1_h, b1_ref), (g2_h, g2_ref), (b2_h, b2_ref))
    norm_copies = [load(src, dst) for src, dst in pairs]

    barrier = pltpu.get_barrier_semaphore()
    far = {"sp": (sp + 31 + 2 * core) % 32, "tp": x}
    zfar, yfar = device(z + 2, y, core, x), device(z, y + 2, core, x)
    friends = (sister, right, left, across, yup, ydown, zup, zdown, far, zfar, yfar)
    for friend in friends:
        pl.semaphore_signal(barrier, inc=1, device_id=friend, device_id_type=MESH)
    with jax.named_scope("barrier"):
        pl.semaphore_wait(barrier, len(friends))

    links = Links(send, recv)
    halo = [links.take() for _ in range(2)]

    seed = links.take()
    seeds = ((right, 3), (left, 1), (across, 2))
    body_cols = pl.ds(XPART, 2048 - XPART)
    ow_copy.wait()
    for target, place in seeds:
        src = oww.at[0, z, y, core, :, body_cols]
        links.start(src, oww.at[place, z, y, core, :, body_cols], seed, target)
    xids = [links.take() for _ in range(4)]

    def xpart(place, ci, zs=ALL):
        return oww.at[place, zs, :, ci, :, pl.ds(0, XPART)]

    def xstart():
        src = xpart(0, core)
        links.start(src, xpart(3, core), xids[0], right)
        links.start(src, xpart(1, core), xids[1], left)

    def xpass():
        links.arrived(xpart(3, core), xids[0], right)
        near = xpart(3, core, pl.ds(0, 2))
        again = lambda place, zs=ALL: lambda: xpart(place, core, zs)
        links.start(near, xpart(2, core, pl.ds(0, 2)), xids[2], right, again(3, pl.ds(0, 2)))
        links.arrived(xpart(1, core), xids[1], left)
        near = xpart(1, core, pl.ds(2, 2))
        links.start(near, xpart(2, core, pl.ds(2, 2)), xids[3], left, again(1, pl.ds(2, 2)))
        links.start(xpart(3, core), xpart(3, core), ow_all, sister, again(3))
        links.start(xpart(1, core), xpart(1, core), ow_all, sister, again(1))

    def xshare():
        links.arrived(xpart(2, core, pl.ds(0, 2)), xids[2], right)
        links.arrived(xpart(2, core, pl.ds(2, 2)), xids[3], left)
        links.start(xpart(2, core), xpart(2, core), ow_all, sister)

    kv_copy.wait()
    last, start = pl.ds(1024, WINDOW), pl.ds(WINDOW, WINDOW)
    links.start(kvv.at[:, last, :], kvv.at[:, pl.ds(0, WINDOW), :], halo[0], later)
    links.start(kvv.at[:, start, :], kvv.at[:, pl.ds(1024 + WINDOW, WINDOW), :], halo[1], earlier)
    xstart()

    def ow_part(half, flip):
        def part_at(one, two, ci, sub):
            zi, yi = (two, one) if flip else (one, two)
            wide = (2048 - XPART) // 2
            at = XPART + half * wide
            if sub is not None:
                first = (wide + 128) // 256 * 128
                at, wide = at + sub * first, wide - first if sub else first
            return oww.at[pl.ds(1, 3), zi, yi, ci, :, pl.ds(at, wide)]

        return part_at

    def wide_part(buffer):
        def make(half, flip):
            def part_at(one, two, ci, sub):
                zi, yi = (two, one) if flip else (one, two)
                span = pl.ds(0, 64) if sub is None else pl.ds(sub * 32, 32)
                return buffer.at[zi, yi, ci, span, pl.ds(half * 1024, 1024)]

            return part_at

        return make

    def spread(make, common, zfar=None, yfar=None):
        return (
            Spread(links, make(0, False), z, y, core, (zup, zdown, yup, ydown), sister, common, zfar),
            Spread(links, make(1, True), y, z, core, (yup, ydown, zup, zdown), sister, common, yfar),
        )

    ow_all, up_all, dn_near, dn_far = (links.take() for _ in range(4))
    outs = spread(ow_part, (ow_all, ow_all), zfar, yfar)
    ups = spread(wide_part(upw), (up_all, up_all))
    downs = spread(wide_part(dnw), (dn_near, dn_far))

    def run(name, pair, step):
        with jax.named_scope(f"{name}{step}"):
            for one in pair:
                getattr(one, f"step{step}")()

    def seeded():
        with jax.named_scope("seed"):
            links.arrived(oww.at[pl.ds(1, 3), z, y, core, :, body_cols], seed, right)
        run("outs", outs, 1)

    def complete(name, half, ident):
        with jax.named_scope(f"{name}7"):
            links.arrived(half, ident, sister)

    up_copy.wait()
    run("ups", ups, 1)
    dn_copy.wait()
    seeded()
    q_copy.wait()
    sink_copy.wait()
    span = BLOCK + 2 * WINDOW
    iota_r = lax.broadcasted_iota(jnp.int32, (BLOCK, span), 0)
    iota_c = lax.broadcasted_iota(jnp.int32, (BLOCK, span), 1)

    def block_copy(index, half, step, target):
        return pltpu.make_async_remote_copy(
            src_ref=att.at[index],
            dst_ref=attr.at[half, :, pl.ds(aligned(3 - step, 512), 512)],
            send_sem=asend.at[half, step],
            recv_sem=arecv.at[half, step],
            device_id=target,
            device_id_type=MESH,
        )

    events = {
        1: lambda: (run("outs", outs, 2), run("outs", outs, 3), run("ups", ups, 2))[2],
        3: xpass,
        5: lambda: (run("outs", outs, 4), run("downs", downs, 1))[1],
        6: lambda: run("ups", ups, 3),
    }

    def attend(index, carry):
        half, step = index // 4, index % 4
        owner = (x + 1 + step) % 4
        block = 2 * owner + half

        @pl.when(block == 0)
        def _():
            links.arrived(kvv.at[:, pl.ds(0, WINDOW), :], halo[0], later)

        @pl.when(block == 7)
        def _():
            links.arrived(kvv.at[:, pl.ds(1024 + WINDOW, WINDOW), :], halo[1], earlier)

        begin = aligned(block, BLOCK)
        pos = iota_c + (sp * 1024 + block * BLOCK - WINDOW)
        gap = iota_c - iota_r
        valid = (gap >= 0) & (gap <= 2 * WINDOW) & (pos >= 0) & (pos < total)
        bias[...] = jnp.where(valid, 0.0, -jnp.inf)
        for kv in range(4):
            lanes = slice(kv * HEAD_DIM, (kv + 1) * HEAD_DIM)
            keys = kvv[0, pl.ds(begin, span), lanes]
            pair = [
                qv[pl.ds(begin, BLOCK), slice(h * HEAD_DIM, (h + 1) * HEAD_DIM)]
                for h in (2 * kv, 2 * kv + 1)
            ]
            query = jnp.concatenate(pair, axis=0) * jnp.asarray(HEAD_DIM ** (-0.5), BF16)
            scores[kv] = lax.dot_general(
                query, keys, (((1,), (1,)), ((), ())), preferred_element_type=F32
            )
        for head in range(8):
            rows_of = slice((head % 2) * BLOCK, (head % 2 + 1) * BLOCK)
            score = scores[head // 2, rows_of] + bias[...]
            sink = sink_ref[head]
            top = jnp.maximum(jnp.max(score, axis=-1, keepdims=True), sink)
            expd = jnp.exp(score - top)
            denom = jnp.sum(expd, axis=-1, keepdims=True) + jnp.exp(sink - top)
            weights[head // 2, rows_of] = expd.astype(BF16)
            scale[head // 2, rows_of] = jnp.broadcast_to(1.0 / denom, (BLOCK, HEAD_DIM))
        for kv in range(4):
            lanes = slice(kv * HEAD_DIM, (kv + 1) * HEAD_DIM)
            values = kvv[1, pl.ds(begin, span), lanes]
            mixed = jnp.dot(weights[kv], values, preferred_element_type=F32) * scale[kv]
            for sub in range(2):
                head = 2 * kv + sub
                att[index, :, head * HEAD_DIM : (head + 1) * HEAD_DIM] = mixed[
                    sub * BLOCK : (sub + 1) * BLOCK
                ].astype(BF16)

        @pl.when(step < 3)
        def _():
            block_copy(index, half, step, {"sp": sp, "tp": owner}).start()

        @pl.when(step == 3)
        def _():
            attr[half, :, 0:512] = att[index]

        for when, event in events.items():
            pl.when(index == when)(event)
        return carry

    with jax.named_scope("attend"):
        lax.fori_loop(0, 8, attend, 0)

    def peer(step):
        return (right, across, left)[step]

    gather = [[links.take() for _ in range(3)] for _ in range(2)]
    low, high = pl.ds(0, 64), pl.ds(64, 64)

    def project(half):
        for step in range(3):
            block_copy(4 * half + step, half, step, peer(step)).wait_recv()

        def body(n, carry):
            cols = pl.ds(aligned(n, 256), 256)
            weight = oww[:, :, :, :, :, cols].reshape(2048, 256)
            term = jnp.dot(attr[half], weight, preferred_element_type=F32)
            there = slice(half * 128, half * 128 + 128)
            pre[there, cols] = term + resv[there, cols].astype(F32)
            return carry

        lax.fori_loop(0, 8, body, 0, unroll=4)

    def norm_first(half):
        def norm(i, carry):
            some = pl.ds(aligned(i, 32), 32)
            there = pl.ds(pl.multiple_of(half * 128 + i * 32, 32), 32)
            rows[half, 0, some, :] = norm_rows(pre[there, :], g1_ref[...], b1_ref[...])
            return carry

        lax.fori_loop(0, 4, norm, 0, unroll=2)

    def offer(half):
        ids = gather[half]
        links.start(rows.at[half, 0, low], rows.at[half, 3, low], ids[0], right)
        links.start(rows.at[half, 0, high], rows.at[half, 1, high], ids[1], left)
        links.start(rows.at[half, 0, high], rows.at[half, 3, high], ids[2], right)
        links.start(rows.at[half, 0, low], rows.at[half, 1, low], ids[2], left)

    def pass_on(half):
        ids = gather[half]
        links.arrived(rows.at[half, 3, low], ids[0], right)
        links.start(rows.at[half, 3, low], rows.at[half, 2, low], ids[2], right)
        links.arrived(rows.at[half, 1, high], ids[1], left)
        links.start(rows.at[half, 1, high], rows.at[half, 2, high], ids[2], left)

    def gathered(half):
        links.arrived(rows.at[half, pl.ds(1, 2)], gather[half][2], right)

    def up_project(half):
        def body(n, carry):
            cols = pl.ds(aligned(n, 256), 256)
            weight = upw[:, :, :, :, cols].reshape(2048, 256)
            hidden = jnp.dot(
                rows[half].reshape(512, 2048), weight, preferred_element_type=F32
            )
            act[:, cols] = jnp.square(jnp.maximum(hidden, 0.0)).astype(BF16)
            return carry

        lax.fori_loop(0, 8, body, 0, unroll=4)

    def scoped(name, phase, half):
        with jax.named_scope(f"{name}{half}"):
            phase(half)

    scatter = [[links.take() for _ in range(3)] for _ in range(2)]

    def down_project(half):
        def product(n, some):
            weight = dnw[n // 2, pl.ds((n % 2) * 2, 2)].reshape(256, 2048)
            return lax.dot_general(some, weight, (((1,), (1,)), ((), ())), preferred_element_type=F32)

        ids = scatter[half]

        def spread_out(cols):
            links.start(part.at[half, 1, low, cols], rin.at[half, 0, :, cols], ids[0], right)
            links.start(part.at[half, 1, high, cols], rin.at[half, 1, :, cols], ids[1], left)
            links.start(part.at[half, 0, high, cols], rfin.at[half, 0, high, cols], ids[2], right)

        def body(n, carry):
            cols = pl.ds(aligned(n, 256), 256)
            term = product(n, act[128:384, :])
            part[half, 0, :, cols] = term[0:128].astype(BF16)
            part[half, 1, :, cols] = term[128:256].astype(BF16)
            return carry

        def tile(n):
            body(n, 0)
            spread_out(pl.ds(aligned(n, 256), 256))

        if half:
            lax.fori_loop(0, 8, body, 0, unroll=4)
            spread_out(ALL)
        else:
            there = (y + 2) % 4 // 2
            for hop in (0, 1, 3):
                tile((z + hop) % 4 * 2 + 1 - there)
            run("downs", downs, 6)
            complete("downs", dnw.at[0, :, 1 - core], dn_far)
            for hop in (0, 1, 3):
                tile((z + hop) % 4 * 2 + there)
            for pair in range(2):
                tile((z + 2) % 4 * 2 + pair)
        def body(n, carry):
            cols = pl.ds(aligned(n, 256), 256)
            some = jnp.concatenate([act[384:512, :], act[0:128, :]], axis=0)
            term = product(n, some)
            part[half, 2, :, cols] = term[0:128].astype(BF16)
            own[half, :, cols] = term[128:256]
            return carry

        lax.fori_loop(0, 8, body, 0, unroll=4)
        links.start(part.at[half, 2, low], rfin.at[half, 1, low], ids[2], left)

    def join(half):
        ids = scatter[half]
        for side, (target, index, at) in enumerate(((right, 0, 0), (left, 2, 64))):
            links.arrived(rin.at[half, side], ids[side], target)
            span = pl.ds(at, 64)
            part[half, index, span, :] = (
                part[half, index, span, :].astype(F32) + rin[half, side].astype(F32)
            ).astype(BF16)
            links.start(
                part.at[half, index, span], rfin.at[half, side, span], ids[2], target
            )

    def final(half):
        links.arrived(rfin.at[half], scatter[half][2], right)

        def norm(i, carry):
            some = pl.ds(aligned(i, 32), 32)
            value = rows[half, 0, some, :].astype(F32) + own[half, some, :]
            value = value + rfin[half, 0, some, :].astype(F32)
            value = value + rfin[half, 1, some, :].astype(F32)
            there = pl.ds(pl.multiple_of(half * 128 + i * 32, 32), 32)
            out_ref[there, :] = norm_rows(value, g2_ref[...], b2_ref[...])
            return carry

        lax.fori_loop(0, 4, norm, 0, unroll=2)

    run("outs", outs, 5)
    run("outs", outs, 6)
    with jax.named_scope("xshare"):
        xshare()
    complete("outs", oww.at[pl.ds(1, 3), :, :, 1 - core], ow_all)
    res_copy.wait()
    for copy in norm_copies:
        copy.wait()
    scoped("project", project, 0)
    scoped("norm_first", norm_first, 0)
    offer(0)
    scoped("project", project, 1)
    scoped("norm_first", norm_first, 1)
    run("downs", downs, 2)
    run("ups", ups, 4)
    scoped("pass_on", pass_on, 0)
    offer(1)
    run("ups", ups, 5)
    run("downs", downs, 3)
    run("ups", ups, 6)
    complete("ups", upw.at[:, :, 1 - core], up_all)
    scoped("gathered", gathered, 0)
    run("downs", downs, 4)
    scoped("up_project", up_project, 0)
    run("downs", downs, 5)
    scoped("pass_on", pass_on, 1)
    complete("near", dnw.at[pl.ds(0, 3), :, 1 - core], dn_near)
    scoped("down_project", down_project, 0)
    scoped("gathered", gathered, 1)
    scoped("up_project", up_project, 1)
    scoped("join", join, 0)
    scoped("down_project", down_project, 1)
    scoped("final", final, 0)
    scoped("join", join, 1)
    for half in range(2):
        for step in range(3):
            block_copy(4 * half + step, half, step, peer(step)).wait_send()
    links.finish(2)
    scoped("final", final, 1)
    with jax.named_scope("finish"):
        links.finish()


def on_device(res, q, kv, sink, ow, g1, b1, up, dn, g2, b2):
    total = q.shape[0] * lax.axis_size("sp")
    hbm = pl.BlockSpec(memory_space=pltpu.HBM)
    vmem = pl.BlockSpec(memory_space=pltpu.VMEM)
    return pl.pallas_call(
        functools.partial(layer_kernel, total),
        in_specs=[hbm] * 11,
        out_specs=vmem,
        out_shape=pltpu.VMEM((256, 2048), BF16),
        scratch_shapes=[
            pltpu.VMEM((1024, 512), BF16),
            pltpu.VMEM((2, 1024 + 2 * WINDOW, 256), BF16),
            pltpu.VMEM((8, 128, 512), BF16),
            pltpu.VMEM((2, 128, 2048), BF16),
            pltpu.VMEM((256, 2048), BF16),
            pltpu.VMEM((4, 4, 4, 2, 16, 2048), BF16),
            pltpu.VMEM((4, 4, 2, 64, 2048), BF16),
            pltpu.VMEM((4, 4, 2, 64, 2048), BF16),
            pltpu.VMEM((2, 4, 128, 2048), BF16),
            pltpu.VMEM((512, 2048), BF16),
            pltpu.VMEM((256, 2048), F32),
            pltpu.VMEM((2, 3, 128, 2048), BF16),
            pltpu.VMEM((2, 128, 2048), F32),
            pltpu.VMEM((2, 2, 64, 2048), BF16),
            pltpu.VMEM((2, 2, 128, 2048), BF16),
            pltpu.VMEM((BLOCK, BLOCK + 2 * WINDOW), F32),
            pltpu.VMEM((4, 2 * BLOCK, BLOCK + 2 * WINDOW), F32),
            pltpu.VMEM((4, 2 * BLOCK, BLOCK + 2 * WINDOW), BF16),
            pltpu.VMEM((4, 2 * BLOCK, HEAD_DIM), F32),
            pltpu.SMEM((8,), F32),
            pltpu.VMEM((1, 2048), F32),
            pltpu.VMEM((1, 2048), F32),
            pltpu.VMEM((1, 2048), F32),
            pltpu.VMEM((1, 2048), F32),
            pltpu.SemaphoreType.DMA((12,)),
            pltpu.SemaphoreType.DMA((SENDS,)),
            pltpu.SemaphoreType.DMA((83,)),
            pltpu.SemaphoreType.DMA((2, 3)),
            pltpu.SemaphoreType.DMA((2, 3)),
        ],
        compiler_params=pltpu.CompilerParams(
            collective_id=0, has_side_effects=True, vmem_limit_bytes=62 * 2**20
        ),
        cost_estimate=pl.CostEstimate(
            flops=2 * 10**10, bytes_accessed=24 * 2**20, transcendentals=4 * 10**6
        ),
        name="layer",
    )(
        res, q, kv, sink, ow.reshape(4, 4, 2, 16, 2048), g1.reshape(1, -1), b1.reshape(1, -1),
        up, dn.T, g2.reshape(1, -1), b2.reshape(1, -1),
    )


def solution(mesh):
    return jax.shard_map(
        on_device,
        mesh=mesh,
        in_specs=(
            P(("sp", "tp"), None),
            P("sp", "tp"),
            P(None, "sp", "tp"),
            P("tp"),
            P("tp", None),
            P(),
            P(),
            P("sp", "tp"),
            P("tp", "sp"),
            P(),
            P(),
        ),
        out_specs=P(("sp", "tp"), None),
        check_vma=False,
    )
```

```python
import functools

import jax
import jax.numpy as jnp
from jax import lax
from jax.experimental import pallas as pl
from jax.experimental.pallas import tpu as pltpu
from jax.sharding import PartitionSpec as P

HEAD_DIM = 64
WINDOW = 128
BLOCK = 128
XPART = 768
SENDS = 56
MESH = pl.DeviceIdType.MESH
F32 = jnp.float32
BF16 = jnp.bfloat16
ALL = slice(None)


def norm_rows(values, gain, bias):
    mean = jnp.mean(values, axis=-1, keepdims=True)
    centred = values - mean
    variance = jnp.mean(centred * centred, axis=-1, keepdims=True)
    return (centred * lax.rsqrt(variance + 1e-06) * gain + bias).astype(BF16)


def aligned(index, size):
    return pl.multiple_of(index * size, size)


class Links:
    def __init__(self, send, recv):
        self.send, self.recv, self.count, self.started = send, recv, 0, []
        self.turn = 0

    def take(self):
        self.count += 1
        return self.count - 1

    def copy(self, src, dst, ident, target, slot=0):
        return pltpu.make_async_remote_copy(
            src_ref=src,
            dst_ref=dst,
            send_sem=self.send.at[slot],
            recv_sem=self.recv.at[ident],
            device_id=target,
            device_id_type=MESH,
        )

    def slot(self):
        slot = self.turn % SENDS
        self.turn += 1
        if self.turn > SENDS:
            self.left(self.started.pop(0))
        return slot

    def left(self, entry):
        again, ident, target, slot = entry
        src = again()
        self.copy(src, src, ident, target, slot).wait_send()

    def start(self, src, dst, ident, target, again=None):
        slot = self.slot()
        self.copy(src, dst, ident, target, slot).start()
        self.started.append((again or (lambda: src), ident, target, slot))

    def arrived(self, dst, ident, target):
        self.copy(dst, dst, ident, target).wait_recv()

    def finish(self, keep=0):
        while len(self.started) > keep:
            self.left(self.started.pop(0))


class Spread:
    def __init__(self, links, part, first, second, core, peers, sister, common, opposite=None):
        self.links, self.part, self.core, self.sister = links, part, core, sister
        self.opposite, self.common = opposite, common
        self.own1, self.own2 = first, second
        self.up1, self.down1, self.up2, self.down2 = peers
        self.ids = [links.take() for _ in range(7)]
        self.near1 = [(first + hop) % 4 for hop in (3, 1, 2)]
        self.near2 = [(second + hop) % 4 for hop in (3, 1, 2)]

    def at(self, one, two, sub=None, core=None):
        return self.part(one, two, self.core if core is None else core, sub)

    def push(self, ident, target, one, two, sub=None):
        place = self.at(one, two, sub)
        self.links.start(place, place, self.ids[ident], target, lambda: self.at(one, two, sub))

    def share(self, two, sub=None, far=False):
        slot, ident = self.links.slot(), self.common[far]
        for one in range(4):
            place = self.at(one, two, sub)
            self.links.copy(place, place, ident, self.sister, slot).start()
        entry = (lambda: self.at(ALL, two, sub), ident, self.sister, slot)
        self.links.started.append(entry)

    def pull(self, ident, target, one, two, sub=None, core=None):
        self.links.arrived(self.at(one, two, sub, core), self.ids[ident], target)

    def step1(self):
        self.push(0, self.up1, self.own1, self.own2)
        self.push(1, self.down1, self.own1, self.own2)
        if self.opposite is not None:
            self.push(2, self.opposite, self.own1, self.own2)

    def step2(self):
        before, after, across = self.near1
        if self.opposite is not None:
            self.pull(0, self.up1, before, self.own2)
            self.pull(1, self.down1, after, self.own2)
            self.pull(2, self.opposite, across, self.own2)
            return
        self.pull(0, self.up1, before, self.own2)
        self.push(2, self.up1, before, self.own2, 0)
        self.pull(1, self.down1, after, self.own2)
        self.push(2, self.down1, after, self.own2, 1)

    def step3(self):
        across = self.near1[2]
        if self.opposite is None:
            self.pull(2, self.up1, across, self.own2)
        self.push(3, self.up2, ALL, self.own2, 0)
        self.push(4, self.down2, ALL, self.own2, 1)
        self.push(6, self.up2, ALL, self.own2, 1)
        self.push(6, self.down2, ALL, self.own2, 0)
        self.share(self.own2)

    def step4(self):
        before, after, _ = self.near2
        self.pull(3, self.up2, ALL, before, 0)
        self.push(5, self.up2, ALL, before, 0)
        self.pull(4, self.down2, ALL, after, 1)
        self.push(5, self.down2, ALL, after, 1)
        self.share(before, 0)
        self.share(after, 1)

    def step5(self):
        before, after, _ = self.near2
        self.pull(6, self.up2, ALL, before)
        self.share(before, 1)
        self.share(after, 0)

    def step6(self):
        across = self.near2[2]
        self.pull(5, self.up2, ALL, across)
        self.share(across, far=True)


def layer_kernel(
    total, res_h, q_h, kv_h, sink_h, ow_h, g1_h, b1_h, up_h, dn_h, g2_h, b2_h, out_ref,
    qv, kvv, att, attr, resv, oww, upw, dnw, rows, act, pre, part, own, rin, rfin, bias, scores, weights, scale,
    sink_ref, g1_ref, b1_ref, g2_ref, b2_ref, local, send, recv, asend, arecv,
):
    sp, x = lax.axis_index("sp"), lax.axis_index("tp")
    core, chip = sp % 2, sp // 2
    y, z = chip % 4, chip // 4

    def device(zi, yi, ci, xi):
        return {"sp": ((zi % 4) * 4 + yi % 4) * 2 + ci, "tp": xi % 4}

    sister = device(z, y, 1 - core, x)
    right, left, across = (device(z, y, core, x + d) for d in (1, 3, 2))
    yup, ydown = device(z, y + 1, core, x), device(z, y + 3, core, x)
    zup, zdown = device(z + 1, y, core, x), device(z + 3, y, core, x)
    later, earlier = {"sp": (sp + 1) % 32, "tp": x}, {"sp": (sp + 31) % 32, "tp": x}

    loads = []

    def load(src, dst):
        copy = pltpu.make_async_copy(src, dst, local.at[len(loads)])
        copy.start()
        loads.append(copy)
        return copy

    ow_copy = load(ow_h, oww.at[0])
    kv_copy = load(kv_h, kvv.at[:, pl.ds(WINDOW, 1024), :])
    q_copy = load(q_h, qv)
    up_copy = load(up_h, upw.at[z, y, core])
    dn_copy = load(dn_h, dnw.at[z, y, core])
    sink_copy = load(sink_h, sink_ref)
    res_copy = load(res_h, resv)
    pairs = ((g1_h, g1_ref), (b1_h, b1_ref), (g2_h, g2_ref), (b2_h, b2_ref))
    norm_copies = [load(src, dst) for src, dst in pairs]

    barrier = pltpu.get_barrier_semaphore()
    far = {"sp": (sp + 31 + 2 * core) % 32, "tp": x}
    zfar, yfar = device(z + 2, y, core, x), device(z, y + 2, core, x)
    friends = (sister, right, left, across, yup, ydown, zup, zdown, far, zfar, yfar)
    for friend in friends:
        pl.semaphore_signal(barrier, inc=1, device_id=friend, device_id_type=MESH)
    with jax.named_scope("barrier"):
        pl.semaphore_wait(barrier, len(friends))

    links = Links(send, recv)
    halo = [links.take() for _ in range(2)]

    seed = links.take()
    seeds = ((right, 3), (left, 1), (across, 2))
    body_cols = pl.ds(XPART, 2048 - XPART)
    ow_copy.wait()
    for target, place in seeds:
        src = oww.at[0, z, y, core, :, body_cols]
        links.start(src, oww.at[place, z, y, core, :, body_cols], seed, target)
    xids = [links.take() for _ in range(4)]

    def xpart(place, ci, zs=ALL):
        return oww.at[place, zs, :, ci, :, pl.ds(0, XPART)]

    def xstart():
        src = xpart(0, core)
        links.start(src, xpart(3, core), xids[0], right)
        links.start(src, xpart(1, core), xids[1], left)

    def xpass():
        links.arrived(xpart(3, core), xids[0], right)
        near = xpart(3, core, pl.ds(0, 2))
        again = lambda place, zs=ALL: lambda: xpart(place, core, zs)
        links.start(near, xpart(2, core, pl.ds(0, 2)), xids[2], right, again(3, pl.ds(0, 2)))
        links.arrived(xpart(1, core), xids[1], left)
        near = xpart(1, core, pl.ds(2, 2))
        links.start(near, xpart(2, core, pl.ds(2, 2)), xids[3], left, again(1, pl.ds(2, 2)))
        links.start(xpart(3, core), xpart(3, core), ow_all, sister, again(3))
        links.start(xpart(1, core), xpart(1, core), ow_all, sister, again(1))

    def xshare():
        links.arrived(xpart(2, core, pl.ds(0, 2)), xids[2], right)
        links.arrived(xpart(2, core, pl.ds(2, 2)), xids[3], left)
        links.start(xpart(2, core), xpart(2, core), ow_all, sister)

    kv_copy.wait()
    last, start = pl.ds(1024, WINDOW), pl.ds(WINDOW, WINDOW)
    links.start(kvv.at[:, last, :], kvv.at[:, pl.ds(0, WINDOW), :], halo[0], later)
    links.start(kvv.at[:, start, :], kvv.at[:, pl.ds(1024 + WINDOW, WINDOW), :], halo[1], earlier)
    xstart()

    def ow_part(half, flip):
        def part_at(one, two, ci, sub):
            zi, yi = (two, one) if flip else (one, two)
            wide = (2048 - XPART) // 2
            at = XPART + half * wide
            if sub is not None:
                first = (wide + 128) // 256 * 128
                at, wide = at + sub * first, wide - first if sub else first
            return oww.at[pl.ds(1, 3), zi, yi, ci, :, pl.ds(at, wide)]

        return part_at

    def wide_part(buffer):
        def make(half, flip):
            def part_at(one, two, ci, sub):
                zi, yi = (two, one) if flip else (one, two)
                span = pl.ds(0, 64) if sub is None else pl.ds(sub * 32, 32)
                return buffer.at[zi, yi, ci, span, pl.ds(half * 1024, 1024)]

            return part_at

        return make

    def spread(make, common, zfar=None, yfar=None):
        return (
            Spread(links, make(0, False), z, y, core, (zup, zdown, yup, ydown), sister, common, zfar),
            Spread(links, make(1, True), y, z, core, (yup, ydown, zup, zdown), sister, common, yfar),
        )

    ow_all, up_all, dn_near, dn_far = (links.take() for _ in range(4))
    outs = spread(ow_part, (ow_all, ow_all), zfar, yfar)
    ups = spread(wide_part(upw), (up_all, up_all))
    downs = spread(wide_part(dnw), (dn_near, dn_far))

    def run(name, pair, step):
        with jax.named_scope(f"{name}{step}"):
            for one in pair:
                getattr(one, f"step{step}")()

    def seeded():
        with jax.named_scope("seed"):
            links.arrived(oww.at[pl.ds(1, 3), z, y, core, :, body_cols], seed, right)
        run("outs", outs, 1)

    def complete(name, half, ident):
        with jax.named_scope(f"{name}7"):
            links.arrived(half, ident, sister)

    up_copy.wait()
    run("ups", ups, 1)
    dn_copy.wait()
    seeded()
    q_copy.wait()
    sink_copy.wait()
    span = BLOCK + 2 * WINDOW
    iota_r = lax.broadcasted_iota(jnp.int32, (BLOCK, span), 0)
    iota_c = lax.broadcasted_iota(jnp.int32, (BLOCK, span), 1)

    def block_copy(index, half, step, target):
        return pltpu.make_async_remote_copy(
            src_ref=att.at[index],
            dst_ref=attr.at[half, :, pl.ds(aligned(3 - step, 512), 512)],
            send_sem=asend.at[half, step],
            recv_sem=arecv.at[half, step],
            device_id=target,
            device_id_type=MESH,
        )

    events = {
        1: lambda: (run("outs", outs, 2), run("outs", outs, 3), run("ups", ups, 2))[2],
        3: xpass,
        5: lambda: (run("outs", outs, 4), run("downs", downs, 1))[1],
        6: lambda: run("ups", ups, 3),
    }

    def attend(index, carry):
        half, step = index // 4, index % 4
        owner = (x + 1 + step) % 4
        block = 2 * owner + half

        @pl.when(block == 0)
        def _():
            links.arrived(kvv.at[:, pl.ds(0, WINDOW), :], halo[0], later)

        @pl.when(block == 7)
        def _():
            links.arrived(kvv.at[:, pl.ds(1024 + WINDOW, WINDOW), :], halo[1], earlier)

        begin = aligned(block, BLOCK)
        pos = iota_c + (sp * 1024 + block * BLOCK - WINDOW)
        gap = iota_c - iota_r
        valid = (gap >= 0) & (gap <= 2 * WINDOW) & (pos >= 0) & (pos < total)
        bias[...] = jnp.where(valid, 0.0, -jnp.inf)
        for kv in range(4):
            lanes = slice(kv * HEAD_DIM, (kv + 1) * HEAD_DIM)
            keys = kvv[0, pl.ds(begin, span), lanes]
            pair = [
                qv[pl.ds(begin, BLOCK), slice(h * HEAD_DIM, (h + 1) * HEAD_DIM)]
                for h in (2 * kv, 2 * kv + 1)
            ]
            query = jnp.concatenate(pair, axis=0) * jnp.asarray(HEAD_DIM ** (-0.5), BF16)
            scores[kv] = lax.dot_general(
                query, keys, (((1,), (1,)), ((), ())), preferred_element_type=F32
            )
        for head in range(8):
            rows_of = slice((head % 2) * BLOCK, (head % 2 + 1) * BLOCK)
            score = scores[head // 2, rows_of] + bias[...]
            sink = sink_ref[head]
            top = jnp.maximum(jnp.max(score, axis=-1, keepdims=True), sink)
            expd = jnp.exp(score - top)
            denom = jnp.sum(expd, axis=-1, keepdims=True) + jnp.exp(sink - top)
            weights[head // 2, rows_of] = expd.astype(BF16)
            scale[head // 2, rows_of] = jnp.broadcast_to(1.0 / denom, (BLOCK, HEAD_DIM))
        for kv in range(4):
            lanes = slice(kv * HEAD_DIM, (kv + 1) * HEAD_DIM)
            values = kvv[1, pl.ds(begin, span), lanes]
            mixed = jnp.dot(weights[kv], values, preferred_element_type=F32) * scale[kv]
            for sub in range(2):
                head = 2 * kv + sub
                att[index, :, head * HEAD_DIM : (head + 1) * HEAD_DIM] = mixed[
                    sub * BLOCK : (sub + 1) * BLOCK
                ].astype(BF16)

        @pl.when(step < 3)
        def _():
            block_copy(index, half, step, {"sp": sp, "tp": owner}).start()

        @pl.when(step == 3)
        def _():
            attr[half, :, 0:512] = att[index]

        for when, event in events.items():
            pl.when(index == when)(event)
        return carry

    with jax.named_scope("attend"):
        lax.fori_loop(0, 8, attend, 0)

    def peer(step):
        return (right, across, left)[step]

    gather = [[links.take() for _ in range(3)] for _ in range(2)]
    low, high = pl.ds(0, 64), pl.ds(64, 64)

    def project(half):
        for step in range(3):
            block_copy(4 * half + step, half, step, peer(step)).wait_recv()

        def body(n, carry):
            cols = pl.ds(aligned(n, 256), 256)
            weight = oww[:, :, :, :, :, cols].reshape(2048, 256)
            term = jnp.dot(attr[half], weight, preferred_element_type=F32)
            there = slice(half * 128, half * 128 + 128)
            pre[there, cols] = term + resv[there, cols].astype(F32)
            return carry

        lax.fori_loop(0, 8, body, 0, unroll=4)

    def norm_first(half, parts):
        def norm(i, carry):
            some = pl.ds(aligned(i, 32), 32)
            there = pl.ds(pl.multiple_of(half * 128 + i * 32, 32), 32)
            rows[half, 0, some, :] = norm_rows(pre[there, :], g1_ref[...], b1_ref[...])
            return carry

        lax.fori_loop(*parts, norm, 0, unroll=2)

    def offer(half):
        ids = gather[half]
        norm_first(half, (0, 2))
        links.start(rows.at[half, 0, low], rows.at[half, 3, low], ids[0], right)
        norm_first(half, (2, 4))
        links.start(rows.at[half, 0, high], rows.at[half, 1, high], ids[1], left)
        links.start(rows.at[half, 0, high], rows.at[half, 3, high], ids[2], right)
        links.start(rows.at[half, 0, low], rows.at[half, 1, low], ids[2], left)

    def pass_on(half):
        ids = gather[half]
        links.arrived(rows.at[half, 3, low], ids[0], right)
        links.start(rows.at[half, 3, low], rows.at[half, 2, low], ids[2], right)
        links.arrived(rows.at[half, 1, high], ids[1], left)
        links.start(rows.at[half, 1, high], rows.at[half, 2, high], ids[2], left)

    def gathered(half):
        links.arrived(rows.at[half, pl.ds(1, 2)], gather[half][2], right)

    def up_project(half):
        def body(n, carry):
            cols = pl.ds(aligned(n, 256), 256)
            weight = upw[:, :, :, :, cols].reshape(2048, 256)
            hidden = jnp.dot(
                rows[half].reshape(512, 2048), weight, preferred_element_type=F32
            )
            act[:, cols] = jnp.square(jnp.maximum(hidden, 0.0)).astype(BF16)
            return carry

        lax.fori_loop(0, 8, body, 0, unroll=4)

    def scoped(name, phase, half):
        with jax.named_scope(f"{name}{half}"):
            phase(half)

    scatter = [[links.take() for _ in range(3)] for _ in range(2)]

    def down_project(half):
        def product(n, some):
            weight = dnw[n // 2, pl.ds((n % 2) * 2, 2)].reshape(256, 2048)
            return lax.dot_general(some, weight, (((1,), (1,)), ((), ())), preferred_element_type=F32)

        ids = scatter[half]

        def spread_out(cols):
            links.start(part.at[half, 1, low, cols], rin.at[half, 0, :, cols], ids[0], right)
            links.start(part.at[half, 1, high, cols], rin.at[half, 1, :, cols], ids[1], left)
            links.start(part.at[half, 0, high, cols], rfin.at[half, 0, high, cols], ids[2], right)

        def body(n, carry):
            cols = pl.ds(aligned(n, 256), 256)
            term = product(n, act[128:384, :])
            part[half, 0, :, cols] = term[0:128].astype(BF16)
            part[half, 1, :, cols] = term[128:256].astype(BF16)
            return carry

        def tile(n):
            body(n, 0)
            spread_out(pl.ds(aligned(n, 256), 256))

        if half:
            lax.fori_loop(0, 8, body, 0, unroll=4)
            spread_out(ALL)
        else:
            there = (y + 2) % 4 // 2
            for hop in (0, 1, 3):
                tile((z + hop) % 4 * 2 + 1 - there)
            run("downs", downs, 6)
            complete("downs", dnw.at[0, :, 1 - core], dn_far)
            for hop in (0, 1, 3):
                tile((z + hop) % 4 * 2 + there)
            for pair in range(2):
                tile((z + 2) % 4 * 2 + pair)
        def body(n, carry):
            cols = pl.ds(aligned(n, 256), 256)
            some = jnp.concatenate([act[384:512, :], act[0:128, :]], axis=0)
            term = product(n, some)
            part[half, 2, :, cols] = term[0:128].astype(BF16)
            own[half, :, cols] = term[128:256]
            return carry

        lax.fori_loop(0, 8, body, 0, unroll=4)
        links.start(part.at[half, 2, low], rfin.at[half, 1, low], ids[2], left)

    def join(half):
        ids = scatter[half]
        for side, (target, index, at) in enumerate(((right, 0, 0), (left, 2, 64))):
            links.arrived(rin.at[half, side], ids[side], target)
            span = pl.ds(at, 64)
            part[half, index, span, :] = (
                part[half, index, span, :].astype(F32) + rin[half, side].astype(F32)
            ).astype(BF16)
            links.start(
                part.at[half, index, span], rfin.at[half, side, span], ids[2], target
            )

    def final(half):
        links.arrived(rfin.at[half], scatter[half][2], right)

        def norm(i, carry):
            some = pl.ds(aligned(i, 32), 32)
            value = rows[half, 0, some, :].astype(F32) + own[half, some, :]
            value = value + rfin[half, 0, some, :].astype(F32)
            value = value + rfin[half, 1, some, :].astype(F32)
            there = pl.ds(pl.multiple_of(half * 128 + i * 32, 32), 32)
            out_ref[there, :] = norm_rows(value, g2_ref[...], b2_ref[...])
            return carry

        lax.fori_loop(0, 4, norm, 0, unroll=2)

    run("outs", outs, 5)
    run("outs", outs, 6)
    with jax.named_scope("xshare"):
        xshare()
    complete("outs", oww.at[pl.ds(1, 3), :, :, 1 - core], ow_all)
    res_copy.wait()
    for copy in norm_copies:
        copy.wait()
    scoped("project", project, 0)
    offer(0)
    scoped("project", project, 1)
    run("downs", downs, 2)
    run("ups", ups, 4)
    scoped("pass_on", pass_on, 0)
    offer(1)
    run("ups", ups, 5)
    run("downs", downs, 3)
    run("ups", ups, 6)
    complete("ups", upw.at[:, :, 1 - core], up_all)
    scoped("gathered", gathered, 0)
    run("downs", downs, 4)
    scoped("up_project", up_project, 0)
    run("downs", downs, 5)
    scoped("pass_on", pass_on, 1)
    complete("near", dnw.at[pl.ds(0, 3), :, 1 - core], dn_near)
    scoped("down_project", down_project, 0)
    scoped("gathered", gathered, 1)
    scoped("up_project", up_project, 1)
    scoped("join", join, 0)
    scoped("down_project", down_project, 1)
    scoped("final", final, 0)
    scoped("join", join, 1)
    for half in range(2):
        for step in range(3):
            block_copy(4 * half + step, half, step, peer(step)).wait_send()
    links.finish(2)
    scoped("final", final, 1)
    with jax.named_scope("finish"):
        links.finish()


def on_device(res, q, kv, sink, ow, g1, b1, up, dn, g2, b2):
    total = q.shape[0] * lax.axis_size("sp")
    hbm = pl.BlockSpec(memory_space=pltpu.HBM)
    vmem = pl.BlockSpec(memory_space=pltpu.VMEM)
    return pl.pallas_call(
        functools.partial(layer_kernel, total),
        in_specs=[hbm] * 11,
        out_specs=vmem,
        out_shape=pltpu.VMEM((256, 2048), BF16),
        scratch_shapes=[
            pltpu.VMEM((1024, 512), BF16),
            pltpu.VMEM((2, 1024 + 2 * WINDOW, 256), BF16),
            pltpu.VMEM((8, 128, 512), BF16),
            pltpu.VMEM((2, 128, 2048), BF16),
            pltpu.VMEM((256, 2048), BF16),
            pltpu.VMEM((4, 4, 4, 2, 16, 2048), BF16),
            pltpu.VMEM((4, 4, 2, 64, 2048), BF16),
            pltpu.VMEM((4, 4, 2, 64, 2048), BF16),
            pltpu.VMEM((2, 4, 128, 2048), BF16),
            pltpu.VMEM((512, 2048), BF16),
            pltpu.VMEM((256, 2048), F32),
            pltpu.VMEM((2, 3, 128, 2048), BF16),
            pltpu.VMEM((2, 128, 2048), F32),
            pltpu.VMEM((2, 2, 64, 2048), BF16),
            pltpu.VMEM((2, 2, 128, 2048), BF16),
            pltpu.VMEM((BLOCK, BLOCK + 2 * WINDOW), F32),
            pltpu.VMEM((4, 2 * BLOCK, BLOCK + 2 * WINDOW), F32),
            pltpu.VMEM((4, 2 * BLOCK, BLOCK + 2 * WINDOW), BF16),
            pltpu.VMEM((4, 2 * BLOCK, HEAD_DIM), F32),
            pltpu.SMEM((8,), F32),
            pltpu.VMEM((1, 2048), F32),
            pltpu.VMEM((1, 2048), F32),
            pltpu.VMEM((1, 2048), F32),
            pltpu.VMEM((1, 2048), F32),
            pltpu.SemaphoreType.DMA((12,)),
            pltpu.SemaphoreType.DMA((SENDS,)),
            pltpu.SemaphoreType.DMA((65,)),
            pltpu.SemaphoreType.DMA((2, 3)),
            pltpu.SemaphoreType.DMA((2, 3)),
        ],
        compiler_params=pltpu.CompilerParams(
            collective_id=0, has_side_effects=True, vmem_limit_bytes=62 * 2**20
        ),
        cost_estimate=pl.CostEstimate(
            flops=2 * 10**10, bytes_accessed=24 * 2**20, transcendentals=4 * 10**6
        ),
        name="layer",
    )(
        res, q, kv, sink, ow.reshape(4, 4, 2, 16, 2048), g1.reshape(1, -1), b1.reshape(1, -1),
        up, dn.T, g2.reshape(1, -1), b2.reshape(1, -1),
    )


def solution(mesh):
    return jax.shard_map(
        on_device,
        mesh=mesh,
        in_specs=(
            P(("sp", "tp"), None),
            P("sp", "tp"),
            P(None, "sp", "tp"),
            P("tp"),
            P("tp", None),
            P(),
            P(),
            P("sp", "tp"),
            P("tp", "sp"),
            P(),
            P(),
        ),
        out_specs=P(("sp", "tp"), None),
        check_vma=False,
    )
```
